32 devices in a mesh: ep: 8 (over z, core), tp: 4 (over y, x).
Axes of the slice: x: 2, y: 2, z: 4, core: 2. Of those that a mesh axis runs over, the one named last changes fastest.
Arguments:
- mix_input: bfloat16 [1024, 2048], P('ep'), may hold values from -8 to 8
- expert_input: bfloat16 [1024, 2048], P('ep'), may hold values from -8 to 8
- mix_gain: float32 [2048], replicated, may hold values from 0.1 to 1.9
- moe_gain: float32 [2048], replicated, may hold values from 0.1 to 1.9
- pool_in: bfloat16 [2048, 1024], P(None, 'tp'), may hold values from -0.125 to 0.125
- pool_scale: float32 [1024], P('tp'), may hold values from 0.25 to 10
- pool_gain: float32 [1024], P('tp'), may hold values from 0.1 to 1.9
- pool_out: bfloat16 [1024, 2048], P(None, 'tp'), may hold values from -0.1875 to 0.1875
- route: int32 [1024, 4], P('ep'), may hold values from 0 to 7, all different within a row; in each aligned block of 128 rows (0 to 127, 128 to 255, ...) at most 128 rows name the same one
- route_score: float32 [1024, 4], P('ep'), may hold values from 0.05 to 1
- expert_gate: bfloat16 [8, 2048, 2048], P('ep', None, 'tp'), may hold values from -0.125 to 0.125
- expert_up: bfloat16 [8, 2048, 2048], P('ep', None, 'tp'), may hold values from -0.125 to 0.125
- expert_down: bfloat16 [8, 2048, 2048], P('ep', 'tp'), may hold values from -0.1875 to 0.1875
- shared_gate: bfloat16 [2048, 2048], P(None, 'tp'), may hold values from -0.125 to 0.125
- shared_up: bfloat16 [2048, 2048], P(None, 'tp'), may hold values from -0.125 to 0.125
- shared_down: bfloat16 [2048, 2048], P(None, 'tp'), may hold values from -0.125 to 0.125
Outputs:
- mix_out: bfloat16 [1024, 2048], P('ep', 'tp')
- moe_out: bfloat16 [1024, 2048], P('ep', 'tp')
The draws below stay inside these ranges and needn't reach their ends.
Inputs may be any that keep to these rules, and one draw needn't show every extreme that they name: `route`: each row names 4 different experts. In the rows of one index of ep (aligned blocks of 128 rows) no expert is named more than 128 times, a bound that some block reaches.
All inputs are finite; a program needn't handle non-finite values.
Results may differ from the reference program's by a relative error of at most 0.014.
Values may be sent and summed in bfloat16 or wider, within the bound.
A program may use at most 64 MiB of HBM per device.

```python
import math
import jax
import jax.numpy as jnp
import numpy as np
from jax import lax

D = 2048
POOL = 1024
FE = 2048
FS = 2048
TOP_K = 4
TOK_B = 128
EXPERTS = 8
CAP = 128
TOKENS_A = 1024
TOKENS_B = 1024
N_EP = 8
N_TP = 4


def spread_rows(key, rows, cols):
    keys = jax.random.split(key, 3)
    row_scale = jnp.exp(jax.random.uniform(keys[0], (rows, 1), jnp.float32, math.log(0.3), math.log(3.0)))
    col_scale = jnp.exp(jax.random.uniform(keys[1], (1, cols), jnp.float32, math.log(0.3), math.log(3.0)))
    base = jax.random.normal(keys[2], (rows, cols), jnp.float32)
    return jnp.clip(base * row_scale * col_scale, -8.0, 8.0).astype(jnp.bfloat16)


def draw_mix_input(key, part):
    return spread_rows(jax.random.fold_in(key, 11), TOKENS_A, D)


def draw_expert_input(key, part):
    return spread_rows(jax.random.fold_in(key, 23), TOKENS_B, D)


def draw_pool_scale(key, part):
    channel = jnp.arange(POOL, dtype=jnp.float32) / POOL
    factor = jnp.exp(jax.random.uniform(jax.random.fold_in(key, 37), (POOL,), jnp.float32, math.log(0.5), math.log(2.0)))
    rising = jnp.exp(math.log(6.0) * channel)
    return 0.5 * rising * factor


def with_spikes(values, own_key, source, target, blocks, factor):
    def block_of(axis_at):
        return (jnp.arange(values.shape[axis_at]) // (values.shape[axis_at] // blocks)).reshape((-1,) + (1,) * (values.ndim - 1 - axis_at))

    near = jax.random.permutation(own_key, blocks)[block_of(target)]
    other_side = (block_of(target) + blocks // 2) % blocks
    return jnp.where((block_of(source) == near) | (block_of(source) == other_side), factor * values, values)


def steps_of(own_key, extent, cuts, low, top_value):
    loudness, own = 1.0, jax.random.fold_in(own_key, 6)
    for axis_at, blocks in cuts:
        steps = jnp.exp(jax.random.uniform(jax.random.fold_in(own, axis_at), (blocks,), jnp.float32, low / len(cuts), top_value / len(cuts)))
        loudness = loudness * jnp.repeat(steps, extent[axis_at] // blocks).reshape([-1 if axis == axis_at else 1 for axis in range(len(extent))])
    return loudness


def routed_block(own_key, own, number, rows, number_of, top, reach, slope):
    order = jax.random.permutation(own_key, number_of)
    heavy_load, usual = load_shares(number_of, rows * top, reach, slope, True), load_shares(number_of, rows * top, reach, slope, False)
    places = jnp.arange(number_of)

    def named(tallies, turn):
        used = int((tallies > 0).sum())
        fixed = max(1, used // 4)
        passed = fixed + (places - fixed + turn * (used - fixed)) % max(1, number_of - fixed)
        return jnp.zeros((number_of,), jnp.int32).at[order[jnp.where(places < fixed, places, passed)]].set(jnp.asarray(tallies, jnp.int32))

    tallies = jnp.where(number % 4 == 0, named(heavy_load, number // 4), named(usual, number - number // 4 - 1))
    mixed = jax.random.permutation(jax.random.fold_in(own, 3), number_of)
    source_of, receiver = mixed[0:number_of // 2 * 2:2], mixed[1:number_of // 2 * 2:2]
    slack = jnp.minimum(tallies[source_of] - 1, reach - tallies[receiver]) // 2
    slack = jnp.where((source_of == order[0]) | (receiver == order[0]) | (tallies[receiver] == 0), 0, jnp.maximum(slack, 0))
    passed = jax.random.randint(jax.random.fold_in(own, 4), (number_of // 2,), 0, 1 << 20) % (slack + 1)
    tallies = tallies.at[source_of].add(-passed).at[receiver].add(passed)
    items = jnp.searchsorted(jnp.cumsum(tallies), jnp.arange(rows * top), side="right").astype(jnp.int32)
    grid = items.reshape(top, rows).T
    grid = grid[jax.random.permutation(jax.random.fold_in(own, 1), rows)]
    turn = jax.random.randint(jax.random.fold_in(own, 2), (rows, 1), 0, top)
    return jnp.take_along_axis(grid, (jnp.arange(top)[None, :] + turn) % top, axis=1)


def load_shares(number_of, total, most, skew, full):
    loads = [(1 << 20) // math.isqrt(grade ** skew) + 1 for grade in range(1, number_of + 1)]
    largest = most if full else min(most, max(-(-total // number_of), total * loads[0] // sum(loads)))
    least = 1 if total - largest >= number_of - 1 else 0
    given, rest = [largest] + [least] * (number_of - 1), total - largest - least * (number_of - 1)
    while rest > 0:
        candidates = [i for i in range(1, number_of) if given[i] < largest] or [i for i in range(1, number_of) if given[i] < most]
        mass, budget = sum([loads[i] for i in candidates]), rest
        for i in candidates:
            more = min(most - given[i], max(1, budget * loads[i] // mass), rest)
            given[i] = given[i] + more
            rest = rest - more
    return np.array(given)


def bell_draw(stream_key, shape, spread, bound, pieces=(), kind=jnp.bfloat16):
    values = spread * jax.random.normal(stream_key, shape, jnp.float32)
    if pieces:
        values = values * steps_of(stream_key, shape, pieces, -0.22, 0.18)
    return jnp.clip(values, -bound, bound).astype(kind)


def gaussian_with(own_key, dims, deviation, reach, pieces, heavy, held_as=jnp.bfloat16):
    values = deviation * jax.random.normal(own_key, dims, jnp.float32)
    if pieces:
        values = values * steps_of(own_key, dims, pieces, -0.22, 0.18)
    return jnp.clip(with_spikes(values, jax.random.fold_in(own_key, 3), *heavy), -reach, reach).astype(held_as)


def setup_inputs(seed: int = 0) -> dict:
    arg_keys = jax.random.split(jax.random.key(seed), 17)
    mix_input = draw_mix_input(jax.random.fold_in(arg_keys[16], 71), 0)
    expert_input = draw_expert_input(jax.random.fold_in(arg_keys[16], 71), 0)
    mix_gain = jnp.clip(1.0 + 0.18 * jax.random.normal(arg_keys[2], (D,), jnp.float32), 0.1, 1.9)
    moe_gain = jnp.clip(1.0 + 0.18 * jax.random.normal(arg_keys[3], (D,), jnp.float32), 0.1, 1.9)
    pool_in = bell_draw(arg_keys[4], (D, POOL), D ** -0.5, 0.125, ((1, 4),))
    pool_scale = draw_pool_scale(jax.random.fold_in(arg_keys[16], 71), 0)
    pool_gain = jnp.clip(1.0 + 0.18 * jax.random.normal(arg_keys[6], (POOL,), jnp.float32), 0.1, 1.9)
    pool_out = bell_draw(arg_keys[7], (POOL, D), POOL ** -0.5, 0.1875, ((1, 4),))
    route_keys = jax.random.split(jax.random.fold_in(arg_keys[8], 1), TOKENS_B // TOK_B)
    route_turns = jax.random.permutation(jax.random.fold_in(arg_keys[8], 3), TOKENS_B // TOK_B)
    route = jax.vmap(lambda own, number: routed_block(jax.random.fold_in(arg_keys[8], 2), own, number, TOK_B, EXPERTS, TOP_K, CAP, 2))(route_keys, route_turns).reshape((TOKENS_B, TOP_K))
    route_score = jnp.clip(0.05 + 0.95 * jax.random.uniform(arg_keys[9], (TOKENS_B, TOP_K), jnp.float32) ** steps_of(arg_keys[9], (TOKENS_B, TOP_K), ((0, 8),), -0.2, 0.2), 0.05, 1.0)
    expert_gate = bell_draw(arg_keys[10], (EXPERTS, D, FE), D ** -0.5, 0.125, ((0, 8), (2, 4)))
    expert_up = bell_draw(arg_keys[11], (EXPERTS, D, FE), D ** -0.5, 0.125, ((0, 8), (2, 4)))
    expert_down = gaussian_with(arg_keys[12], (EXPERTS, FE, D), FE ** -0.5, 0.1875, ((0, 8), (1, 4)), (1, 2, 4, 2.0))
    shared_gate = bell_draw(arg_keys[13], (D, FS), D ** -0.5, 0.125, ((1, 4),))
    shared_up = bell_draw(arg_keys[14], (D, FS), D ** -0.5, 0.125, ((1, 4),))
    shared_down = bell_draw(arg_keys[15], (FS, D), FS ** -0.5, 0.125, ((1, 4),))
    return {"mix_input": mix_input, "expert_input": expert_input, "mix_gain": mix_gain, "moe_gain": moe_gain, "pool_in": pool_in, "pool_scale": pool_scale, "pool_gain": pool_gain, "pool_out": pool_out, "route": route, "route_score": route_score, "expert_gate": expert_gate, "expert_up": expert_up, "expert_down": expert_down, "shared_gate": shared_gate, "shared_up": shared_up, "shared_down": shared_down}


epsilon = 1e-06
reach_rows = 15
window_widths = (2, 4, 8, 16)

def row_norm(rows, gain):
    values = rows.astype(jnp.float32)
    scale = lax.rsqrt(lax.optimization_barrier(jnp.mean(values * values, axis=-1, keepdims=True)) + epsilon)
    return (values * scale * gain.astype(jnp.float32)).astype(jnp.bfloat16)

def window_means(extended, position, group, n_rows):
    total = jnp.zeros((n_rows, extended.shape[1]), jnp.float32)
    result = jnp.zeros((n_rows, extended.shape[1]), jnp.float32)
    for lag in range(16):
        total = total + extended[reach_rows - lag:reach_rows - lag + n_rows]
        for index, width in enumerate(window_widths):
            if lag + 1 == width:
                count = jnp.minimum(position, float(width))[:, None]
                result = jnp.where(group[None, :] == index, total / count, result)
    return result - extended[reach_rows:]

def reference(mix_input, expert_input, mix_gain, moe_gain, pool_in, pool_scale, pool_gain, pool_out, route, route_score, expert_gate, expert_up, expert_down, shared_gate, shared_up, shared_down):
    mix_norm = row_norm(mix_input, mix_gain)
    pool_input = jnp.dot(mix_norm, pool_in, preferred_element_type=jnp.float32).astype(jnp.bfloat16)
    extended = jnp.concatenate([jnp.zeros((reach_rows, POOL), jnp.float32), pool_input.astype(jnp.float32)], axis=0)
    position = jnp.arange(1, TOKENS_A + 1, dtype=jnp.int32).astype(jnp.float32)
    group = jnp.arange(POOL, dtype=jnp.int32) // (POOL // 4)
    scaled = window_means(extended, position, group, TOKENS_A) * pool_scale
    pooled_norm = (scaled * lax.rsqrt(lax.optimization_barrier(jnp.mean(scaled * scaled, axis=1, keepdims=True)) + epsilon) * pool_gain).astype(jnp.bfloat16)
    mix_out = jnp.dot(pooled_norm, pool_out, preferred_element_type=jnp.float32).astype(jnp.bfloat16)
    moe_norm = row_norm(expert_input, moe_gain)
    weights = 2.5 * route_score / lax.optimization_barrier(jnp.sum(route_score, axis=1, keepdims=True))
    most_rows = CAP * N_EP

    def one_expert(routed, expert):
        hit = route == expert
        taken = jnp.any(hit, axis=1)
        order = jnp.argsort(jnp.where(taken, 0, 1).astype(jnp.int32), stable=True)[:most_rows].astype(jnp.int32)
        live = taken[order]
        rows = moe_norm[order]
        gate = jnp.dot(rows, expert_gate[expert], preferred_element_type=jnp.float32)
        upper = jnp.dot(rows, expert_up[expert], preferred_element_type=jnp.float32)
        hidden = (jax.nn.silu(gate) * upper).astype(jnp.bfloat16)
        blocks = hidden.reshape(most_rows, N_TP, FE // N_TP).astype(jnp.float32)
        down = expert_down[expert].reshape(N_TP, FE // N_TP, D).astype(jnp.float32)
        partial_value = jnp.einsum('rpf,pfd->rpd', blocks, down).astype(jnp.bfloat16)
        result = lax.optimization_barrier(jnp.sum(partial_value.astype(jnp.float32), axis=1)).astype(jnp.bfloat16)
        factor = lax.optimization_barrier(jnp.sum(jnp.where(hit, weights, 0.0), axis=1))[order] * live
        routed = routed.at[order].add(result.astype(jnp.float32) * factor[:, None])
        return (routed, None)
    routed, _ = lax.scan(one_expert, jnp.zeros((TOKENS_B, D), jnp.float32), jnp.arange(EXPERTS, dtype=jnp.int32))
    shared_hidden = (jax.nn.silu(jnp.dot(moe_norm, shared_gate, preferred_element_type=jnp.float32)) * jnp.dot(moe_norm, shared_up, preferred_element_type=jnp.float32)).astype(jnp.bfloat16)
    shared = jnp.dot(shared_hidden, shared_down, preferred_element_type=jnp.float32)
    moe_out = (routed + shared).astype(jnp.bfloat16)
    return (mix_out, moe_out)
```

```python
import jax
import jax.numpy as jnp
from jax import lax
from jax.experimental import pallas as pl
from jax.experimental.pallas import tpu as pltpu
from jax.sharding import PartitionSpec as P

epsilon = 1e-06
reach_rows = 15
window_widths = (2, 4, 8, 16)


def shifted(block, axis, distance):
    devices = range(lax.axis_size(axis))
    route = [(i - distance, i) for i in devices if i - distance in devices]
    return lax.ppermute(block, axis, route)


def row_norm(rows, gain):
    values = rows.astype(jnp.float32)
    scale = lax.rsqrt(jnp.mean(values * values, axis=-1, keepdims=True) + epsilon)
    return (values * scale * gain).astype(jnp.bfloat16)


def window_means(extended, position, group, n_rows):
    total = jnp.zeros((n_rows, extended.shape[1]), jnp.float32)
    result = jnp.zeros((n_rows, extended.shape[1]), jnp.float32)
    for lag in range(16):
        total = total + extended[reach_rows - lag : reach_rows - lag + n_rows]
        for index, width in enumerate(window_widths):
            if lag + 1 == width:
                count = jnp.minimum(position, float(width))[:, None]
                result = jnp.where(group[None, :] == index, total / count, result)
    return result - extended[reach_rows:]


def serve(sending, expert_gate, expert_up, expert_down):
    arrived = lax.all_to_all(sending, "ep", split_axis=0, concat_axis=0, tiled=True)
    gate = jnp.einsum("send,edf->senf", arrived, expert_gate, preferred_element_type=jnp.float32)
    upper = jnp.einsum("send,edf->senf", arrived, expert_up, preferred_element_type=jnp.float32)
    hidden = (jax.nn.silu(gate) * upper).astype(jnp.bfloat16)
    term = jnp.einsum("senf,efd->send", hidden, expert_down, preferred_element_type=jnp.float32)
    summed = lax.psum_scatter(term.astype(jnp.bfloat16), "tp", scatter_dimension=3, tiled=True)
    return lax.all_to_all(summed, "ep", split_axis=0, concat_axis=0, tiled=True)


def on_device(
    mix_input,
    expert_input,
    mix_gain,
    moe_gain,
    pool_in,
    pool_scale,
    pool_gain,
    pool_out,
    route,
    route_score,
    expert_gate,
    expert_up,
    expert_down,
    shared_gate,
    shared_up,
    shared_down,
):
    tok_rows = mix_input.shape[0]
    channels = pool_in.shape[1]
    pool_width = channels * lax.axis_size("tp")
    mix_norm = row_norm(mix_input, mix_gain)
    pool_input = jnp.dot(mix_norm, pool_in, preferred_element_type=jnp.float32).astype(jnp.bfloat16)
    before = shifted(pool_input[tok_rows - reach_rows :], "ep", 1)
    extended = jnp.concatenate([before, pool_input], axis=0).astype(jnp.float32)
    position = (lax.axis_index("ep") * tok_rows + jnp.arange(tok_rows, dtype=jnp.int32) + 1).astype(
        jnp.float32
    )
    channel_ids = lax.axis_index("tp") * channels + jnp.arange(channels, dtype=jnp.int32)
    group = channel_ids // (pool_width // 4)
    scaled = window_means(extended, position, group, tok_rows) * pool_scale
    squares = lax.psum(jnp.sum(scaled * scaled, axis=1), "tp")
    pooled_norm = (scaled * lax.rsqrt(squares / pool_width + epsilon)[:, None] * pool_gain).astype(
        jnp.bfloat16
    )
    moe_norm = row_norm(expert_input, moe_gain)
    shared_hidden = (
        jax.nn.silu(jnp.dot(moe_norm, shared_gate, preferred_element_type=jnp.float32))
        * jnp.dot(moe_norm, shared_up, preferred_element_type=jnp.float32)
    ).astype(jnp.bfloat16)
    pooled_all, shared_all = (
        lax.all_gather(pooled_norm, "tp", axis=1, tiled=True),
        lax.all_gather(shared_hidden, "tp", axis=1, tiled=True),
    )
    mix_out = jnp.dot(pooled_all, pool_out, preferred_element_type=jnp.float32).astype(jnp.bfloat16)
    shared_part = jnp.dot(shared_all, shared_down, preferred_element_type=jnp.float32)
    n_tok, top = route.shape
    local_experts = expert_gate.shape[0]
    experts = local_experts * lax.axis_size("ep")
    capacity = 2 * n_tok * top // experts
    flat_route = route.reshape(-1)
    table = (flat_route[:, None] == jnp.arange(experts, dtype=jnp.int32)[None, :]).astype(jnp.int32)
    ranks = jnp.sum((jnp.cumsum(table, axis=0) - table) * table, axis=1)
    slot = flat_route * capacity + ranks
    owner = (
        jnp.full((experts * capacity,), n_tok, jnp.int32)
        .at[slot]
        .set(jnp.arange(n_tok * top, dtype=jnp.int32) // top)
    )
    padded_rows = jnp.concatenate(
        [moe_norm, jnp.zeros((1, moe_norm.shape[1]), jnp.bfloat16)], axis=0
    )
    outgoing = padded_rows[owner].reshape(
        lax.axis_size("ep"), local_experts, capacity, moe_norm.shape[1]
    )
    middle = capacity // 2
    first = serve(outgoing[:, :, :middle], expert_gate, expert_up, expert_down)
    second = serve(outgoing[:, :, middle:], expert_gate, expert_up, expert_down)
    returned = jnp.concatenate([first, second], axis=2)
    back_rows = returned.reshape(experts * capacity, returned.shape[3])
    picked = back_rows[slot].reshape(n_tok, top, returned.shape[3]).astype(jnp.float32)
    weights = 2.5 * route_score / jnp.sum(route_score, axis=1, keepdims=True)
    routed = jnp.sum(picked * weights[:, :, None], axis=1)
    moe_out = (routed + shared_part).astype(jnp.bfloat16)
    return (mix_out, moe_out)


MESH = pl.DeviceIdType.MESH


def places():
    ep, tp = lax.axis_index("ep"), lax.axis_index("tp")
    z, core = ep // 2, ep % 2
    y, x = tp // 2, tp % 2
    return ep, tp, z, core, y * 2 + 1 - x, (1 - y) * 2 + x, (1 - y) * 2 + 1 - x


def greet(partners):
    barrier = pltpu.get_barrier_semaphore()
    for partner in partners:
        pl.semaphore_signal(barrier, inc=1, device_id=partner, device_id_type=MESH)
    pl.semaphore_wait(barrier, len(partners))


def aligned(start, size):
    return pl.ds(pl.multiple_of(start * size, size), size)


def gather_kernel(n_ep, m_ref, w_ref, g_ref, wg_ref, *sems):
    (w_s, w_r, z_s, z_r, x_s, x_r, y_s, y_r, dx_s, dx_r, dy_s, dy_r, c_s, c_r) = sems
    ep, tp, z, core, xn, yn, _ = places()
    n_z = n_ep // 2
    rows = m_ref.shape[0]
    cols = m_ref.shape[1] // 4
    half = rows // 2
    greet([((ep + m) % n_ep, tp) for m in range(1, n_ep)] + [(ep, xn), (ep, yn)])

    def send(src, dst, s, r, device):
        copy = pltpu.make_async_remote_copy(
            src_ref=src, dst_ref=dst, send_sem=s, recv_sem=r, device_id=device, device_id_type=MESH
        )
        copy.start()
        return copy

    own_rows = aligned(ep, rows)
    other_core = z * 2 + 1 - core
    order = [k for k in (1, n_z - 1)] + list(range(2, n_z - 1))
    z_copies = {}
    for k in order:
        target = ((z + k) % n_z) * 2 + core
        z_copies[k] = send(
            m_ref.at[:, aligned(tp, cols)],
            g_ref.at[own_rows, aligned(tp, cols)],
            z_s.at[k],
            z_r.at[k],
            (target, tp),
        )
    c_copies = {0: send(m_ref, g_ref.at[own_rows, :], c_s.at[0], c_r.at[0], (other_core, tp))}
    w_copies = [
        send(w_ref, wg_ref.at[ep], w_s.at[m], w_r.at[m], ((ep + m) % n_ep, tp))
        for m in range(1, n_ep)
    ]
    g_ref[own_rows, :] = m_ref[...]
    wg_ref[ep] = w_ref[...]
    x_copies, y_copies, dx_copies, dy_copies = {}, {}, {}, {}

    def block(k):
        return ((z + n_z - k) % n_z) * 2 + core

    def piece(k, quarter):
        return g_ref.at[aligned(block(k), rows), aligned(quarter, cols)]

    def half_piece(k, part, quarter):
        start = pl.multiple_of(block(k) * rows + part * half, half)
        return g_ref.at[pl.ds(start, half), aligned(quarter, cols)]

    def across(k):
        z_copies[k].wait_recv()
        x_copies[k] = send(piece(k, tp), piece(k, tp), x_s.at[k], x_r.at[k], (ep, xn))
        y_copies[k] = send(piece(k, tp), piece(k, tp), y_s.at[k], y_r.at[k], (ep, yn))

    def corner(k):
        x_copies[k].wait_recv()
        dx_copies[k] = send(
            half_piece(k, 0, xn), half_piece(k, 0, xn), dx_s.at[k], dx_r.at[k], (ep, yn)
        )
        y_copies[k].wait_recv()
        dy_copies[k] = send(
            half_piece(k, 1, yn), half_piece(k, 1, yn), dy_s.at[k], dy_r.at[k], (ep, xn)
        )

    def over(k):
        dx_copies[k].wait_recv()
        dy_copies[k].wait_recv()
        whole = g_ref.at[aligned(block(k), rows), :]
        c_copies[k] = send(whole, whole, c_s.at[k], c_r.at[k], (other_core, tp))

    for index in range(len(order) + 2):
        if index < len(order):
            across(order[index])
        if 1 <= index < len(order) + 1:
            corner(order[index - 1])
        if index >= 2:
            over(order[index - 2])
    for k in [0] + order:
        c_copies[k].wait_recv()
    for copy in w_copies:
        copy.wait()
    for group in (z_copies, x_copies, y_copies, dx_copies, dy_copies, c_copies):
        for copy in group.values():
            copy.wait_send()


def gather_rows(moe_norm, dense, n_ep):
    n_z = n_ep // 2
    sems = [pltpu.SemaphoreType.DMA((n_ep,))] * 2 + [pltpu.SemaphoreType.DMA((n_z,))] * 12
    vmem = pl.BlockSpec(memory_space=pltpu.VMEM)
    return pl.pallas_call(
        lambda *refs: gather_kernel(n_ep, *refs),
        out_shape=(
            jax.ShapeDtypeStruct((n_ep * moe_norm.shape[0], moe_norm.shape[1]), jnp.bfloat16),
            jax.ShapeDtypeStruct((n_ep,) + dense.shape, jnp.float32),
        ),
        in_specs=[vmem] * 2,
        out_specs=(vmem, vmem),
        scratch_shapes=sems,
        compiler_params=pltpu.CompilerParams(collective_id=0, has_side_effects=True),
    )(moe_norm, dense)


def reduce_kernel(n_ep, p_ref, sh_ref, po_ref, sq_ref, o_ref, sh_all, po_all, sq_all, *scratch):
    (ca, s, bx, by, qx, qy, r, bz) = scratch[:8]
    (c_s, c_r, dx_s, dx_r, dy_s, dy_r, x_s, x_r, y_s, y_r, z_s, z_r, t_s, t_r) = scratch[8:]
    ep, tp, z, core, xn, yn, dg = places()
    n_z = n_ep // 2
    rows = o_ref.shape[0]
    cols = o_ref.shape[1]
    half = rows // 2
    other_core = z * 2 + 1 - core
    peers = (xn, yn, dg)
    greet(
        [(other_core, tp)]
        + [(((z + k) % n_z) * 2 + core, tp) for k in range(1, n_z)]
        + [(ep, t) for t in peers]
    )

    def send(src, dst, sem_s, sem_r, device):
        copy = pltpu.make_async_remote_copy(
            src_ref=src, dst_ref=dst, send_sem=sem_s, recv_sem=sem_r, device_id=device, device_id_type=MESH
        )
        copy.start()
        return copy

    order = list(range(2, n_z - 1)) + [1, n_z - 1, 0]
    c_copies, dx_copies, dy_copies, x_copies, y_copies, z_copies = {}, {}, {}, {}, {}, {}
    for k in order:
        away = ((z + k) % n_z) * 2 + 1 - core
        c_copies[k] = send(
            p_ref.at[aligned(away, rows), :], ca.at[k], c_s.at[k], c_r.at[k], (other_core, tp)
        )
    low, high = pl.ds(0, half), pl.ds(half, half)

    def first(k):
        c_copies[k].wait_recv()
        mine = ((z + k) % n_z) * 2 + core
        s[k] = (
            p_ref[aligned(mine, rows), :].astype(jnp.float32) + ca[k].astype(jnp.float32)
        ).astype(jnp.bfloat16)
        dx_copies[k] = send(
            s.at[k, low, aligned(dg, cols)], bx.at[k], dx_s.at[k], dx_r.at[k], (ep, xn)
        )
        dy_copies[k] = send(
            s.at[k, high, aligned(dg, cols)], by.at[k], dy_s.at[k], dy_r.at[k], (ep, yn)
        )

    def second(k):
        dx_copies[k].wait_recv()
        s[k, low, aligned(yn, cols)] = (
            s[k, low, aligned(yn, cols)].astype(jnp.float32) + bx[k].astype(jnp.float32)
        ).astype(jnp.bfloat16)
        y_copies[k] = send(
            s.at[k, :, aligned(yn, cols)], qy.at[k], y_s.at[k], y_r.at[k], (ep, yn)
        )
        dy_copies[k].wait_recv()
        s[k, high, aligned(xn, cols)] = (
            s[k, high, aligned(xn, cols)].astype(jnp.float32) + by[k].astype(jnp.float32)
        ).astype(jnp.bfloat16)
        x_copies[k] = send(
            s.at[k, :, aligned(xn, cols)], qx.at[k], x_s.at[k], x_r.at[k], (ep, xn)
        )

    def third(k):
        x_copies[k].wait_recv()
        y_copies[k].wait_recv()
        total = (
            s[k, :, aligned(tp, cols)].astype(jnp.float32)
            + qx[k].astype(jnp.float32)
            + qy[k].astype(jnp.float32)
        )
        if k == 0:
            o_ref[...] = total
        else:
            r[k] = total.astype(jnp.bfloat16)
            target = ((z + k) % n_z) * 2 + core
            z_copies[k] = send(r.at[k], bz.at[k], z_s.at[k], z_r.at[k], (target, tp))

    t_copies = []
    for index in range(n_z + 2):
        if index < n_z:
            first(order[index])
        if 1 <= index < n_z + 1:
            second(order[index - 1])
        if index == n_z:
            for number, t in enumerate(peers):
                pairs = (
                    (sh_ref, sh_all.at[:, aligned(tp, sh_ref.shape[1])]),
                    (po_ref, po_all.at[:, aligned(tp, po_ref.shape[1])]),
                    (sq_ref, sq_all.at[tp]),
                )
                for kind, (src, dst) in enumerate(pairs):
                    t_copies.append(
                        send(src, dst, t_s.at[number, kind], t_r.at[number, kind], (ep, t))
                    )
        if index >= 2:
            third(order[index - 2])
    sh_all[:, aligned(tp, sh_ref.shape[1])] = sh_ref[...]
    po_all[:, aligned(tp, po_ref.shape[1])] = po_ref[...]
    sq_all[tp] = sq_ref[...]
    for k in order[:-1]:
        z_copies[k].wait_recv()
        o_ref[...] += bz[k].astype(jnp.float32)
    for copy in t_copies:
        copy.wait()
    for group in (c_copies, dx_copies, dy_copies, x_copies, y_copies, z_copies):
        for copy in group.values():
            copy.wait_send()


def reduce_rows(weighted, shared_hidden, pooled, squares, n_ep, n_tp):
    n_z = n_ep // 2
    rows, width = weighted.shape[0] // n_ep, weighted.shape[1]
    cols = width // n_tp
    half = rows // 2
    bf16 = jnp.bfloat16
    vmem = pl.BlockSpec(memory_space=pltpu.VMEM)
    scratch = [
        pltpu.VMEM((n_z, rows, width), bf16),
        pltpu.VMEM((n_z, rows, width), bf16),
        pltpu.VMEM((n_z, half, cols), bf16),
        pltpu.VMEM((n_z, half, cols), bf16),
        pltpu.VMEM((n_z, rows, cols), bf16),
        pltpu.VMEM((n_z, rows, cols), bf16),
        pltpu.VMEM((n_z, rows, cols), bf16),
        pltpu.VMEM((n_z, rows, cols), bf16),
    ]
    sems = [pltpu.SemaphoreType.DMA((n_z,))] * 12 + [pltpu.SemaphoreType.DMA((3, 3))] * 2
    return pl.pallas_call(
        lambda *refs: reduce_kernel(n_ep, *refs),
        out_shape=(
            jax.ShapeDtypeStruct((rows, cols), jnp.float32),
            jax.ShapeDtypeStruct((rows, n_tp * shared_hidden.shape[1]), bf16),
            jax.ShapeDtypeStruct((rows, n_tp * pooled.shape[1]), bf16),
            jax.ShapeDtypeStruct((n_tp,) + squares.shape, jnp.float32),
        ),
        in_specs=[vmem] * 4,
        out_specs=(vmem,) * 4,
        scratch_shapes=scratch + sems,
        compiler_params=pltpu.CompilerParams(
            collective_id=1, has_side_effects=True, vmem_limit_bytes=40 << 20
        ),
    )(weighted, shared_hidden, pooled, squares)


def dense_on_device(
    mix_input,
    expert_input,
    mix_gain,
    moe_gain,
    pool_in,
    pool_scale,
    pool_gain,
    pool_out,
    route,
    route_score,
    expert_gate,
    expert_up,
    expert_down,
    shared_gate,
    shared_up,
    shared_down,
):
    n_ep, n_tp = lax.axis_size("ep"), lax.axis_size("tp")
    me = lax.axis_index("ep")
    tok_rows = mix_input.shape[0]
    channels = pool_in.shape[1]
    pool_width = channels * n_tp
    f32 = jnp.float32

    moe_norm = row_norm(expert_input, moe_gain)
    weights = 2.5 * route_score / jnp.sum(route_score, axis=1, keepdims=True)
    experts = jnp.arange(n_ep, dtype=jnp.int32)
    dense = jnp.sum(
        jnp.where(route.T[None, :, :] == experts[:, None, None], weights.T[None, :, :], 0.0), axis=1
    )
    mix_norm = row_norm(mix_input, mix_gain)
    pool_input = jnp.dot(mix_norm, pool_in, preferred_element_type=f32).astype(jnp.bfloat16)
    before = shifted(pool_input[tok_rows - reach_rows :], "ep", 1)
    all_rows, all_weights = gather_rows(moe_norm, dense, n_ep)

    extended = jnp.concatenate([before, pool_input], axis=0).astype(f32)
    position = (me * tok_rows + jnp.arange(tok_rows, dtype=jnp.int32) + 1).astype(f32)
    channel_ids = lax.axis_index("tp") * channels + jnp.arange(channels, dtype=jnp.int32)
    group = channel_ids // (pool_width // 4)
    scaled = window_means(extended, position, group, tok_rows) * pool_scale
    squares = jnp.sum(scaled * scaled, axis=1)[None, :]
    pooled = (scaled * pool_gain).astype(jnp.bfloat16)
    shared_hidden = (
        jax.nn.silu(jnp.dot(moe_norm, shared_gate, preferred_element_type=f32))
        * jnp.dot(moe_norm, shared_up, preferred_element_type=f32)
    ).astype(jnp.bfloat16)

    factor = lax.dynamic_index_in_dim(all_weights, me, axis=1, keepdims=False).reshape(-1, 1)
    gate = jnp.dot(all_rows, expert_gate[0], preferred_element_type=f32)
    upper = jnp.dot(all_rows, expert_up[0], preferred_element_type=f32)
    hidden = (jax.nn.silu(gate) * upper).astype(jnp.bfloat16)
    weighted = (jnp.dot(hidden, expert_down[0], preferred_element_type=f32) * factor).astype(
        jnp.bfloat16
    )
    routed, shared_all, pooled_all, squares_all = reduce_rows(
        weighted, shared_hidden, pooled, squares, n_ep, n_tp
    )
    mean = jnp.sum(squares_all, axis=0).reshape(-1, 1) / pool_width
    mix_out = (
        jnp.dot(pooled_all, pool_out, preferred_element_type=f32) * lax.rsqrt(mean + epsilon)
    ).astype(jnp.bfloat16)
    shared_part = jnp.dot(shared_all, shared_down, preferred_element_type=f32)
    return (mix_out, (routed + shared_part).astype(jnp.bfloat16))


def chosen(*arrays):
    route, expert_gate = arrays[8], arrays[10]
    experts = expert_gate.shape[0] * lax.axis_size("ep")
    capacity = 2 * route.shape[0] * route.shape[1] // experts
    square = lax.axis_size("tp") == 4 and lax.axis_size("ep") >= 6
    if capacity == route.shape[0] and expert_gate.shape[0] == 1 and square:
        return dense_on_device(*arrays)
    return on_device(*arrays)


def solution(mesh):
    return jax.shard_map(
        chosen,
        mesh=mesh,
        in_specs=(
            P("ep", None),
            P("ep", None),
            P(),
            P(),
            P(None, "tp"),
            P("tp"),
            P("tp"),
            P(None, "tp"),
            P("ep", None),
            P("ep", None),
            P("ep", None, "tp"),
            P("ep", None, "tp"),
            P("ep", "tp", None),
            P(None, "tp"),
            P(None, "tp"),
            P(None, "tp"),
        ),
        out_specs=(P("ep", "tp"), P("ep", "tp")),
        check_vma=False,
    )
```

```python
import jax
import jax.numpy as jnp
from jax import lax
from jax.experimental import pallas as pl
from jax.experimental.pallas import tpu as pltpu
from jax.sharding import PartitionSpec as P

epsilon = 1e-06
reach_rows = 15
window_widths = (2, 4, 8, 16)


def shifted(block, axis, distance):
    devices = range(lax.axis_size(axis))
    route = [(i - distance, i) for i in devices if i - distance in devices]
    return lax.ppermute(block, axis, route)


def row_norm(rows, gain):
    values = rows.astype(jnp.float32)
    scale = lax.rsqrt(jnp.mean(values * values, axis=-1, keepdims=True) + epsilon)
    return (values * scale * gain).astype(jnp.bfloat16)


def window_means(extended, position, group, n_rows):
    total = jnp.zeros((n_rows, extended.shape[1]), jnp.float32)
    result = jnp.zeros((n_rows, extended.shape[1]), jnp.float32)
    for lag in range(16):
        total = total + extended[reach_rows - lag : reach_rows - lag + n_rows]
        for index, width in enumerate(window_widths):
            if lag + 1 == width:
                count = jnp.minimum(position, float(width))[:, None]
                result = jnp.where(group[None, :] == index, total / count, result)
    return result - extended[reach_rows:]


def serve(sending, expert_gate, expert_up, expert_down):
    arrived = lax.all_to_all(sending, "ep", split_axis=0, concat_axis=0, tiled=True)
    gate = jnp.einsum("send,edf->senf", arrived, expert_gate, preferred_element_type=jnp.float32)
    upper = jnp.einsum("send,edf->senf", arrived, expert_up, preferred_element_type=jnp.float32)
    hidden = (jax.nn.silu(gate) * upper).astype(jnp.bfloat16)
    term = jnp.einsum("senf,efd->send", hidden, expert_down, preferred_element_type=jnp.float32)
    summed = lax.psum_scatter(term.astype(jnp.bfloat16), "tp", scatter_dimension=3, tiled=True)
    return lax.all_to_all(summed, "ep", split_axis=0, concat_axis=0, tiled=True)


def on_device(
    mix_input,
    expert_input,
    mix_gain,
    moe_gain,
    pool_in,
    pool_scale,
    pool_gain,
    pool_out,
    route,
    route_score,
    expert_gate,
    expert_up,
    expert_down,
    shared_gate,
    shared_up,
    shared_down,
):
    tok_rows = mix_input.shape[0]
    channels = pool_in.shape[1]
    pool_width = channels * lax.axis_size("tp")
    mix_norm = row_norm(mix_input, mix_gain)
    pool_input = jnp.dot(mix_norm, pool_in, preferred_element_type=jnp.float32).astype(jnp.bfloat16)
    before = shifted(pool_input[tok_rows - reach_rows :], "ep", 1)
    extended = jnp.concatenate([before, pool_input], axis=0).astype(jnp.float32)
    position = (lax.axis_index("ep") * tok_rows + jnp.arange(tok_rows, dtype=jnp.int32) + 1).astype(
        jnp.float32
    )
    channel_ids = lax.axis_index("tp") * channels + jnp.arange(channels, dtype=jnp.int32)
    group = channel_ids // (pool_width // 4)
    scaled = window_means(extended, position, group, tok_rows) * pool_scale
    squares = lax.psum(jnp.sum(scaled * scaled, axis=1), "tp")
    pooled_norm = (scaled * lax.rsqrt(squares / pool_width + epsilon)[:, None] * pool_gain).astype(
        jnp.bfloat16
    )
    moe_norm = row_norm(expert_input, moe_gain)
    shared_hidden = (
        jax.nn.silu(jnp.dot(moe_norm, shared_gate, preferred_element_type=jnp.float32))
        * jnp.dot(moe_norm, shared_up, preferred_element_type=jnp.float32)
    ).astype(jnp.bfloat16)
    pooled_all, shared_all = (
        lax.all_gather(pooled_norm, "tp", axis=1, tiled=True),
        lax.all_gather(shared_hidden, "tp", axis=1, tiled=True),
    )
    mix_out = jnp.dot(pooled_all, pool_out, preferred_element_type=jnp.float32).astype(jnp.bfloat16)
    shared_part = jnp.dot(shared_all, shared_down, preferred_element_type=jnp.float32)
    n_tok, top = route.shape
    local_experts = expert_gate.shape[0]
    experts = local_experts * lax.axis_size("ep")
    capacity = 2 * n_tok * top // experts
    flat_route = route.reshape(-1)
    table = (flat_route[:, None] == jnp.arange(experts, dtype=jnp.int32)[None, :]).astype(jnp.int32)
    ranks = jnp.sum((jnp.cumsum(table, axis=0) - table) * table, axis=1)
    slot = flat_route * capacity + ranks
    owner = (
        jnp.full((experts * capacity,), n_tok, jnp.int32)
        .at[slot]
        .set(jnp.arange(n_tok * top, dtype=jnp.int32) // top)
    )
    padded_rows = jnp.concatenate(
        [moe_norm, jnp.zeros((1, moe_norm.shape[1]), jnp.bfloat16)], axis=0
    )
    outgoing = padded_rows[owner].reshape(
        lax.axis_size("ep"), local_experts, capacity, moe_norm.shape[1]
    )
    middle = capacity // 2
    first = serve(outgoing[:, :, :middle], expert_gate, expert_up, expert_down)
    second = serve(outgoing[:, :, middle:], expert_gate, expert_up, expert_down)
    returned = jnp.concatenate([first, second], axis=2)
    back_rows = returned.reshape(experts * capacity, returned.shape[3])
    picked = back_rows[slot].reshape(n_tok, top, returned.shape[3]).astype(jnp.float32)
    weights = 2.5 * route_score / jnp.sum(route_score, axis=1, keepdims=True)
    routed = jnp.sum(picked * weights[:, :, None], axis=1)
    moe_out = (routed + shared_part).astype(jnp.bfloat16)
    return (mix_out, moe_out)


MESH = pl.DeviceIdType.MESH


def places():
    ep, tp = lax.axis_index("ep"), lax.axis_index("tp")
    z, core = ep // 2, ep % 2
    y, x = tp // 2, tp % 2
    return ep, tp, z, core, y * 2 + 1 - x, (1 - y) * 2 + x, (1 - y) * 2 + 1 - x


def greet(partners):
    barrier = pltpu.get_barrier_semaphore()
    for partner in partners:
        pl.semaphore_signal(barrier, inc=1, device_id=partner, device_id_type=MESH)
    pl.semaphore_wait(barrier, len(partners))


def aligned(start, size):
    return pl.ds(pl.multiple_of(start * size, size), size)


def gather_kernel(n_ep, m_ref, w_ref, g_ref, wg_ref, *sems):
    (w_s, w_r, z_s, z_r, x_s, x_r, y_s, y_r, dx_s, dx_r, dy_s, dy_r, c_s, c_r) = sems
    ep, tp, z, core, xn, yn, _ = places()
    n_z = n_ep // 2
    rows = m_ref.shape[0]
    cols = m_ref.shape[1] // 4
    half = rows // 2
    greet([((ep + m) % n_ep, tp) for m in range(1, n_ep)] + [(ep, xn), (ep, yn)])

    def send(src, dst, s, r, device):
        copy = pltpu.make_async_remote_copy(
            src_ref=src, dst_ref=dst, send_sem=s, recv_sem=r, device_id=device, device_id_type=MESH
        )
        copy.start()
        return copy

    own_rows = aligned(ep, rows)
    other_core = z * 2 + 1 - core
    order = [k for k in (1, n_z - 1)] + list(range(2, n_z - 1))
    z_copies = {}
    for k in order:
        target = ((z + k) % n_z) * 2 + core
        z_copies[k] = send(
            m_ref.at[:, aligned(tp, cols)],
            g_ref.at[own_rows, aligned(tp, cols)],
            z_s.at[k],
            z_r.at[k],
            (target, tp),
        )
    c_copies = {0: send(m_ref, g_ref.at[own_rows, :], c_s.at[0], c_r.at[0], (other_core, tp))}
    w_copies = [
        send(w_ref, wg_ref.at[ep], w_s.at[m], w_r.at[m], ((ep + m) % n_ep, tp))
        for m in range(1, n_ep)
    ]
    g_ref[own_rows, :] = m_ref[...]
    wg_ref[ep] = w_ref[...]
    x_copies, y_copies, dx_copies, dy_copies = {}, {}, {}, {}

    def block(k):
        return ((z + n_z - k) % n_z) * 2 + core

    def piece(k, quarter):
        return g_ref.at[aligned(block(k), rows), aligned(quarter, cols)]

    def half_piece(k, part, quarter):
        start = pl.multiple_of(block(k) * rows + part * half, half)
        return g_ref.at[pl.ds(start, half), aligned(quarter, cols)]

    def across(k):
        z_copies[k].wait_recv()
        x_copies[k] = send(piece(k, tp), piece(k, tp), x_s.at[k], x_r.at[k], (ep, xn))
        y_copies[k] = send(piece(k, tp), piece(k, tp), y_s.at[k], y_r.at[k], (ep, yn))

    def corner(k):
        x_copies[k].wait_recv()
        dx_copies[k] = send(
            half_piece(k, 0, xn), half_piece(k, 0, xn), dx_s.at[k], dx_r.at[k], (ep, yn)
        )
        y_copies[k].wait_recv()
        dy_copies[k] = send(
            half_piece(k, 1, yn), half_piece(k, 1, yn), dy_s.at[k], dy_r.at[k], (ep, xn)
        )

    def over(k):
        dx_copies[k].wait_recv()
        dy_copies[k].wait_recv()
        whole = g_ref.at[aligned(block(k), rows), :]
        c_copies[k] = send(whole, whole, c_s.at[k], c_r.at[k], (other_core, tp))

    for index in range(len(order) + 2):
        if index < len(order):
            across(order[index])
        if 1 <= index < len(order) + 1:
            corner(order[index - 1])
        if index >= 2:
            over(order[index - 2])
    for k in [0] + order:
        c_copies[k].wait_recv()
    for copy in w_copies:
        copy.wait()
    for group in (z_copies, x_copies, y_copies, dx_copies, dy_copies, c_copies):
        for copy in group.values():
            copy.wait_send()


def gather_rows(moe_norm, dense, n_ep):
    n_z = n_ep // 2
    sems = [pltpu.SemaphoreType.DMA((n_ep,))] * 2 + [pltpu.SemaphoreType.DMA((n_z,))] * 12
    vmem = pl.BlockSpec(memory_space=pltpu.VMEM)
    return pl.pallas_call(
        lambda *refs: gather_kernel(n_ep, *refs),
        out_shape=(
            jax.ShapeDtypeStruct((n_ep * moe_norm.shape[0], moe_norm.shape[1]), jnp.bfloat16),
            jax.ShapeDtypeStruct((n_ep,) + dense.shape, jnp.float32),
        ),
        in_specs=[vmem] * 2,
        out_specs=(vmem, vmem),
        scratch_shapes=sems,
        compiler_params=pltpu.CompilerParams(collective_id=0, has_side_effects=True, vmem_limit_bytes=16 << 20),
    )(moe_norm, dense)


def reduce_kernel(n_ep, p_ref, sh_ref, po_ref, sq_ref, o_ref, sh_all, po_all, sq_all, *scratch):
    (ca, s, bx, by, qx, qy, r, bz) = scratch[:8]
    (c_s, c_r, dx_s, dx_r, dy_s, dy_r, x_s, x_r, y_s, y_r, z_s, z_r, t_s, t_r) = scratch[8:]
    ep, tp, z, core, xn, yn, dg = places()
    n_z = n_ep // 2
    rows = o_ref.shape[0]
    cols = o_ref.shape[1]
    half = rows // 2
    other_core = z * 2 + 1 - core
    peers = (xn, yn, dg)
    greet(
        [(other_core, tp)]
        + [(((z + k) % n_z) * 2 + core, tp) for k in range(1, n_z)]
        + [(ep, t) for t in peers]
    )

    def send(src, dst, sem_s, sem_r, device):
        copy = pltpu.make_async_remote_copy(
            src_ref=src, dst_ref=dst, send_sem=sem_s, recv_sem=sem_r, device_id=device, device_id_type=MESH
        )
        copy.start()
        return copy

    order = list(range(2, n_z - 1)) + [1, n_z - 1, 0]
    c_copies, dx_copies, dy_copies, x_copies, y_copies, z_copies = {}, {}, {}, {}, {}, {}
    for k in order:
        away = ((z + k) % n_z) * 2 + 1 - core
        c_copies[k] = send(
            p_ref.at[aligned(away, rows), :], ca.at[k], c_s.at[k], c_r.at[k], (other_core, tp)
        )
    low, high = pl.ds(0, half), pl.ds(half, half)

    def first(k):
        c_copies[k].wait_recv()
        mine = ((z + k) % n_z) * 2 + core
        s[k] = (
            p_ref[aligned(mine, rows), :].astype(jnp.float32) + ca[k].astype(jnp.float32)
        ).astype(jnp.bfloat16)
        dx_copies[k] = send(
            s.at[k, low, aligned(dg, cols)], bx.at[k], dx_s.at[k], dx_r.at[k], (ep, xn)
        )
        dy_copies[k] = send(
            s.at[k, high, aligned(dg, cols)], by.at[k], dy_s.at[k], dy_r.at[k], (ep, yn)
        )

    def second(k):
        dx_copies[k].wait_recv()
        s[k, low, aligned(yn, cols)] = (
            s[k, low, aligned(yn, cols)].astype(jnp.float32) + bx[k].astype(jnp.float32)
        ).astype(jnp.bfloat16)
        y_copies[k] = send(
            s.at[k, :, aligned(yn, cols)], qy.at[k], y_s.at[k], y_r.at[k], (ep, yn)
        )
        dy_copies[k].wait_recv()
        s[k, high, aligned(xn, cols)] = (
            s[k, high, aligned(xn, cols)].astype(jnp.float32) + by[k].astype(jnp.float32)
        ).astype(jnp.bfloat16)
        x_copies[k] = send(
            s.at[k, :, aligned(xn, cols)], qx.at[k], x_s.at[k], x_r.at[k], (ep, xn)
        )

    def third(k):
        x_copies[k].wait_recv()
        y_copies[k].wait_recv()
        total = (
            s[k, :, aligned(tp, cols)].astype(jnp.float32)
            + qx[k].astype(jnp.float32)
            + qy[k].astype(jnp.float32)
        )
        if k == 0:
            o_ref[...] = total
        else:
            r[k] = total.astype(jnp.bfloat16)
            target = ((z + k) % n_z) * 2 + core
            z_copies[k] = send(r.at[k], bz.at[k], z_s.at[k], z_r.at[k], (target, tp))

    t_copies = []
    for index in range(n_z + 2):
        if index < n_z:
            first(order[index])
        if 1 <= index < n_z + 1:
            second(order[index - 1])
        if index == n_z:
            for number, t in enumerate(peers):
                pairs = (
                    (sh_ref, sh_all.at[:, aligned(tp, sh_ref.shape[1])]),
                    (po_ref, po_all.at[:, aligned(tp, po_ref.shape[1])]),
                    (sq_ref, sq_all.at[tp]),
                )
                for kind, (src, dst) in enumerate(pairs):
                    t_copies.append(
                        send(src, dst, t_s.at[number, kind], t_r.at[number, kind], (ep, t))
                    )
        if index >= 2:
            third(order[index - 2])
    sh_all[:, aligned(tp, sh_ref.shape[1])] = sh_ref[...]
    po_all[:, aligned(tp, po_ref.shape[1])] = po_ref[...]
    sq_all[tp] = sq_ref[...]
    for k in order[:-1]:
        z_copies[k].wait_recv()
        o_ref[...] += bz[k].astype(jnp.float32)
    for copy in t_copies:
        copy.wait()
    for group in (c_copies, dx_copies, dy_copies, x_copies, y_copies, z_copies):
        for copy in group.values():
            copy.wait_send()


def reduce_rows(weighted, shared_hidden, pooled, squares, n_ep, n_tp):
    n_z = n_ep // 2
    rows, width = weighted.shape[0] // n_ep, weighted.shape[1]
    cols = width // n_tp
    half = rows // 2
    bf16 = jnp.bfloat16
    vmem = pl.BlockSpec(memory_space=pltpu.VMEM)
    scratch = [
        pltpu.VMEM((n_z, rows, width), bf16),
        pltpu.VMEM((n_z, rows, width), bf16),
        pltpu.VMEM((n_z, half, cols), bf16),
        pltpu.VMEM((n_z, half, cols), bf16),
        pltpu.VMEM((n_z, rows, cols), bf16),
        pltpu.VMEM((n_z, rows, cols), bf16),
        pltpu.VMEM((n_z, rows, cols), bf16),
        pltpu.VMEM((n_z, rows, cols), bf16),
    ]
    sems = [pltpu.SemaphoreType.DMA((n_z,))] * 12 + [pltpu.SemaphoreType.DMA((3, 3))] * 2
    return pl.pallas_call(
        lambda *refs: reduce_kernel(n_ep, *refs),
        out_shape=(
            jax.ShapeDtypeStruct((rows, cols), jnp.float32),
            jax.ShapeDtypeStruct((rows, n_tp * shared_hidden.shape[1]), bf16),
            jax.ShapeDtypeStruct((rows, n_tp * pooled.shape[1]), bf16),
            jax.ShapeDtypeStruct((n_tp,) + squares.shape, jnp.float32),
        ),
        in_specs=[vmem] * 4,
        out_specs=(vmem,) * 4,
        scratch_shapes=scratch + sems,
        compiler_params=pltpu.CompilerParams(
            collective_id=1, has_side_effects=True, vmem_limit_bytes=16 << 20
        ),
    )(weighted, shared_hidden, pooled, squares)


def dense_on_device(
    mix_input,
    expert_input,
    mix_gain,
    moe_gain,
    pool_in,
    pool_scale,
    pool_gain,
    pool_out,
    route,
    route_score,
    expert_gate,
    expert_up,
    expert_down,
    shared_gate,
    shared_up,
    shared_down,
):
    n_ep, n_tp = lax.axis_size("ep"), lax.axis_size("tp")
    me = lax.axis_index("ep")
    tok_rows = mix_input.shape[0]
    channels = pool_in.shape[1]
    pool_width = channels * n_tp
    f32 = jnp.float32

    moe_norm = row_norm(expert_input, moe_gain)
    weights = 2.5 * route_score / jnp.sum(route_score, axis=1, keepdims=True)
    experts = jnp.arange(n_ep, dtype=jnp.int32)
    dense = jnp.sum(
        jnp.where(route.T[None, :, :] == experts[:, None, None], weights.T[None, :, :], 0.0), axis=1
    )
    mix_norm = row_norm(mix_input, mix_gain)
    pool_input = jnp.dot(mix_norm, pool_in, preferred_element_type=f32).astype(jnp.bfloat16)
    before = shifted(pool_input[tok_rows - reach_rows :], "ep", 1)
    all_rows, all_weights = gather_rows(moe_norm, dense, n_ep)

    extended = jnp.concatenate([before, pool_input], axis=0).astype(f32)
    position = (me * tok_rows + jnp.arange(tok_rows, dtype=jnp.int32) + 1).astype(f32)
    channel_ids = lax.axis_index("tp") * channels + jnp.arange(channels, dtype=jnp.int32)
    group = channel_ids // (pool_width // 4)
    scaled = window_means(extended, position, group, tok_rows) * pool_scale
    squares = jnp.sum(scaled * scaled, axis=1)[None, :]
    pooled = (scaled * pool_gain).astype(jnp.bfloat16)
    shared_hidden = (
        jax.nn.silu(jnp.dot(moe_norm, shared_gate, preferred_element_type=f32))
        * jnp.dot(moe_norm, shared_up, preferred_element_type=f32)
    ).astype(jnp.bfloat16)

    factor = lax.dynamic_index_in_dim(all_weights, me, axis=1, keepdims=False).reshape(-1, 1)
    gate = jnp.dot(all_rows, expert_gate[0], preferred_element_type=f32)
    upper = jnp.dot(all_rows, expert_up[0], preferred_element_type=f32)
    hidden = (jax.nn.silu(gate) * upper * factor).astype(jnp.bfloat16)
    weighted = jnp.dot(hidden, expert_down[0], preferred_element_type=f32).astype(jnp.bfloat16)
    routed, shared_all, pooled_all, squares_all = reduce_rows(
        weighted, shared_hidden, pooled, squares, n_ep, n_tp
    )
    mean = jnp.sum(squares_all, axis=0).reshape(-1, 1) / pool_width
    mix_out = (
        jnp.dot(pooled_all, pool_out, preferred_element_type=f32) * lax.rsqrt(mean + epsilon)
    ).astype(jnp.bfloat16)
    shared_part = jnp.dot(shared_all, shared_down, preferred_element_type=f32)
    return (mix_out, (routed + shared_part).astype(jnp.bfloat16))


def chosen(*arrays):
    route, expert_gate = arrays[8], arrays[10]
    experts = expert_gate.shape[0] * lax.axis_size("ep")
    capacity = 2 * route.shape[0] * route.shape[1] // experts
    square = lax.axis_size("tp") == 4 and lax.axis_size("ep") >= 6
    if capacity == route.shape[0] and expert_gate.shape[0] == 1 and square:
        return dense_on_device(*arrays)
    return on_device(*arrays)


def solution(mesh):
    return jax.shard_map(
        chosen,
        mesh=mesh,
        in_specs=(
            P("ep", None),
            P("ep", None),
            P(),
            P(),
            P(None, "tp"),
            P("tp"),
            P("tp"),
            P(None, "tp"),
            P("ep", None),
            P("ep", None),
            P("ep", None, "tp"),
            P("ep", None, "tp"),
            P("ep", "tp", None),
            P(None, "tp"),
            P(None, "tp"),
            P(None, "tp"),
        ),
        out_specs=(P("ep", "tp"), P("ep", "tp")),
        check_vma=False,
    )
```

```python
import jax
import jax.numpy as jnp
from jax import lax
from jax.experimental import pallas as pl
from jax.experimental.pallas import tpu as pltpu
from jax.sharding import PartitionSpec as P

epsilon = 1e-06
reach_rows = 15
window_widths = (2, 4, 8, 16)


def shifted(block, axis, distance):
    devices = range(lax.axis_size(axis))
    route = [(i - distance, i) for i in devices if i - distance in devices]
    return lax.ppermute(block, axis, route)


def row_norm(rows, gain):
    values = rows.astype(jnp.float32)
    scale = lax.rsqrt(jnp.mean(values * values, axis=-1, keepdims=True) + epsilon)
    return (values * scale * gain).astype(jnp.bfloat16)


def window_means(extended, position, group, n_rows):
    total = jnp.zeros((n_rows, extended.shape[1]), jnp.float32)
    result = jnp.zeros((n_rows, extended.shape[1]), jnp.float32)
    for lag in range(16):
        total = total + extended[reach_rows - lag : reach_rows - lag + n_rows]
        for index, width in enumerate(window_widths):
            if lag + 1 == width:
                count = jnp.minimum(position, float(width))[:, None]
                result = jnp.where(group[None, :] == index, total / count, result)
    return result - extended[reach_rows:]


def serve(sending, expert_gate, expert_up, expert_down):
    arrived = lax.all_to_all(sending, "ep", split_axis=0, concat_axis=0, tiled=True)
    gate = jnp.einsum("send,edf->senf", arrived, expert_gate, preferred_element_type=jnp.float32)
    upper = jnp.einsum("send,edf->senf", arrived, expert_up, preferred_element_type=jnp.float32)
    hidden = (jax.nn.silu(gate) * upper).astype(jnp.bfloat16)
    term = jnp.einsum("senf,efd->send", hidden, expert_down, preferred_element_type=jnp.float32)
    summed = lax.psum_scatter(term.astype(jnp.bfloat16), "tp", scatter_dimension=3, tiled=True)
    return lax.all_to_all(summed, "ep", split_axis=0, concat_axis=0, tiled=True)


def on_device(
    mix_input,
    expert_input,
    mix_gain,
    moe_gain,
    pool_in,
    pool_scale,
    pool_gain,
    pool_out,
    route,
    route_score,
    expert_gate,
    expert_up,
    expert_down,
    shared_gate,
    shared_up,
    shared_down,
):
    tok_rows = mix_input.shape[0]
    channels = pool_in.shape[1]
    pool_width = channels * lax.axis_size("tp")
    mix_norm = row_norm(mix_input, mix_gain)
    pool_input = jnp.dot(mix_norm, pool_in, preferred_element_type=jnp.float32).astype(jnp.bfloat16)
    before = shifted(pool_input[tok_rows - reach_rows :], "ep", 1)
    extended = jnp.concatenate([before, pool_input], axis=0).astype(jnp.float32)
    position = (lax.axis_index("ep") * tok_rows + jnp.arange(tok_rows, dtype=jnp.int32) + 1).astype(
        jnp.float32
    )
    channel_ids = lax.axis_index("tp") * channels + jnp.arange(channels, dtype=jnp.int32)
    group = channel_ids // (pool_width // 4)
    scaled = window_means(extended, position, group, tok_rows) * pool_scale
    squares = lax.psum(jnp.sum(scaled * scaled, axis=1), "tp")
    pooled_norm = (scaled * lax.rsqrt(squares / pool_width + epsilon)[:, None] * pool_gain).astype(
        jnp.bfloat16
    )
    moe_norm = row_norm(expert_input, moe_gain)
    shared_hidden = (
        jax.nn.silu(jnp.dot(moe_norm, shared_gate, preferred_element_type=jnp.float32))
        * jnp.dot(moe_norm, shared_up, preferred_element_type=jnp.float32)
    ).astype(jnp.bfloat16)
    pooled_all, shared_all = (
        lax.all_gather(pooled_norm, "tp", axis=1, tiled=True),
        lax.all_gather(shared_hidden, "tp", axis=1, tiled=True),
    )
    mix_out = jnp.dot(pooled_all, pool_out, preferred_element_type=jnp.float32).astype(jnp.bfloat16)
    shared_part = jnp.dot(shared_all, shared_down, preferred_element_type=jnp.float32)
    n_tok, top = route.shape
    local_experts = expert_gate.shape[0]
    experts = local_experts * lax.axis_size("ep")
    capacity = 2 * n_tok * top // experts
    flat_route = route.reshape(-1)
    table = (flat_route[:, None] == jnp.arange(experts, dtype=jnp.int32)[None, :]).astype(jnp.int32)
    ranks = jnp.sum((jnp.cumsum(table, axis=0) - table) * table, axis=1)
    slot = flat_route * capacity + ranks
    owner = (
        jnp.full((experts * capacity,), n_tok, jnp.int32)
        .at[slot]
        .set(jnp.arange(n_tok * top, dtype=jnp.int32) // top)
    )
    padded_rows = jnp.concatenate(
        [moe_norm, jnp.zeros((1, moe_norm.shape[1]), jnp.bfloat16)], axis=0
    )
    outgoing = padded_rows[owner].reshape(
        lax.axis_size("ep"), local_experts, capacity, moe_norm.shape[1]
    )
    middle = capacity // 2
    first = serve(outgoing[:, :, :middle], expert_gate, expert_up, expert_down)
    second = serve(outgoing[:, :, middle:], expert_gate, expert_up, expert_down)
    returned = jnp.concatenate([first, second], axis=2)
    back_rows = returned.reshape(experts * capacity, returned.shape[3])
    picked = back_rows[slot].reshape(n_tok, top, returned.shape[3]).astype(jnp.float32)
    weights = 2.5 * route_score / jnp.sum(route_score, axis=1, keepdims=True)
    routed = jnp.sum(picked * weights[:, :, None], axis=1)
    moe_out = (routed + shared_part).astype(jnp.bfloat16)
    return (mix_out, moe_out)


MESH = pl.DeviceIdType.MESH


def places():
    ep, tp = lax.axis_index("ep"), lax.axis_index("tp")
    z, core = ep // 2, ep % 2
    y, x = tp // 2, tp % 2
    return ep, tp, z, core, y * 2 + 1 - x, (1 - y) * 2 + x, (1 - y) * 2 + 1 - x


def greet(partners):
    barrier = pltpu.get_barrier_semaphore()
    for partner in partners:
        pl.semaphore_signal(barrier, inc=1, device_id=partner, device_id_type=MESH)
    pl.semaphore_wait(barrier, len(partners))


def aligned(start, size):
    return pl.ds(pl.multiple_of(start * size, size), size)


def gather_kernel(n_ep, m_ref, w_ref, sg_ref, su_ref, g_ref, wg_ref, sh_ref, *sems):
    (w_s, w_r, z_s, z_r, x_s, x_r, y_s, y_r, dx_s, dx_r, dy_s, dy_r, c_s, c_r) = sems
    ep, tp, z, core, xn, yn, _ = places()
    n_z = n_ep // 2
    rows = m_ref.shape[0]
    cols = m_ref.shape[1] // 4
    half = rows // 2
    greet([((ep + m) % n_ep, tp) for m in range(1, n_ep)] + [(ep, xn), (ep, yn)])

    def send(src, dst, s, r, device):
        copy = pltpu.make_async_remote_copy(
            src_ref=src, dst_ref=dst, send_sem=s, recv_sem=r, device_id=device, device_id_type=MESH
        )
        copy.start()
        return copy

    own_rows = aligned(ep, rows)
    other_core = z * 2 + 1 - core
    order = [k for k in (1, n_z - 1)] + list(range(2, n_z - 1))
    z_copies = {}
    for k in order:
        target = ((z + k) % n_z) * 2 + core
        z_copies[k] = send(
            m_ref.at[:, aligned(tp, cols)],
            g_ref.at[own_rows, aligned(tp, cols)],
            z_s.at[k],
            z_r.at[k],
            (target, tp),
        )
    c_copies = {0: send(m_ref, g_ref.at[own_rows, :], c_s.at[0], c_r.at[0], (other_core, tp))}
    w_copies = [
        send(w_ref, wg_ref.at[ep], w_s.at[m], w_r.at[m], ((ep + m) % n_ep, tp))
        for m in range(1, n_ep)
    ]
    g_ref[own_rows, :] = m_ref[...]
    wg_ref[ep] = w_ref[...]
    tile = sg_ref.shape[1] // 2

    def shared_tile(index, carry):
        part = aligned(index, tile)
        gate = jnp.dot(m_ref[...], sg_ref[:, part], preferred_element_type=jnp.float32)
        upper = jnp.dot(m_ref[...], su_ref[:, part], preferred_element_type=jnp.float32)
        sh_ref[:, part] = (gate / (1.0 + jnp.exp(-gate)) * upper).astype(jnp.bfloat16)
        return carry

    lax.fori_loop(0, 2, shared_tile, 0)
    x_copies, y_copies, dx_copies, dy_copies = {}, {}, {}, {}

    def block(k):
        return ((z + n_z - k) % n_z) * 2 + core

    def piece(k, quarter):
        return g_ref.at[aligned(block(k), rows), aligned(quarter, cols)]

    def half_piece(k, part, quarter):
        start = pl.multiple_of(block(k) * rows + part * half, half)
        return g_ref.at[pl.ds(start, half), aligned(quarter, cols)]

    def across(k):
        z_copies[k].wait_recv()
        x_copies[k] = send(piece(k, tp), piece(k, tp), x_s.at[k], x_r.at[k], (ep, xn))
        y_copies[k] = send(piece(k, tp), piece(k, tp), y_s.at[k], y_r.at[k], (ep, yn))

    def corner(k):
        x_copies[k].wait_recv()
        dx_copies[k] = send(
            half_piece(k, 0, xn), half_piece(k, 0, xn), dx_s.at[k], dx_r.at[k], (ep, yn)
        )
        y_copies[k].wait_recv()
        dy_copies[k] = send(
            half_piece(k, 1, yn), half_piece(k, 1, yn), dy_s.at[k], dy_r.at[k], (ep, xn)
        )

    def over(k):
        dx_copies[k].wait_recv()
        dy_copies[k].wait_recv()
        whole = g_ref.at[aligned(block(k), rows), :]
        c_copies[k] = send(whole, whole, c_s.at[k], c_r.at[k], (other_core, tp))

    for index in range(len(order) + 2):
        if index < len(order):
            across(order[index])
        if 1 <= index < len(order) + 1:
            corner(order[index - 1])
        if index >= 2:
            over(order[index - 2])
    for k in [0] + order:
        c_copies[k].wait_recv()
    for copy in w_copies:
        copy.wait()
    for group in (z_copies, x_copies, y_copies, dx_copies, dy_copies, c_copies):
        for copy in group.values():
            copy.wait_send()


def gather_rows(moe_norm, dense, shared_gate, shared_up, n_ep):
    n_z = n_ep // 2
    sems = [pltpu.SemaphoreType.DMA((n_ep,))] * 2 + [pltpu.SemaphoreType.DMA((n_z,))] * 12
    vmem = pl.BlockSpec(memory_space=pltpu.VMEM)
    return pl.pallas_call(
        lambda *refs: gather_kernel(n_ep, *refs),
        out_shape=(
            jax.ShapeDtypeStruct((n_ep * moe_norm.shape[0], moe_norm.shape[1]), jnp.bfloat16),
            jax.ShapeDtypeStruct((n_ep,) + dense.shape, jnp.float32),
            jax.ShapeDtypeStruct((moe_norm.shape[0], shared_gate.shape[1]), jnp.bfloat16),
        ),
        in_specs=[vmem] * 4,
        out_specs=(vmem,) * 3,
        scratch_shapes=sems,
        compiler_params=pltpu.CompilerParams(collective_id=0, has_side_effects=True, vmem_limit_bytes=20 << 20),
    )(moe_norm, dense, shared_gate, shared_up)


def reduce_kernel(n_ep, h_ref, down_ref, sh_ref, po_ref, sq_ref, o_ref, sh_all, po_all, sq_all, *scratch):
    (p, ca, s, bx, by, qx, qy, r, bz) = scratch[:9]
    (c_s, c_r, dx_s, dx_r, dy_s, dy_r, x_s, x_r, y_s, y_r, z_s, z_r, t_s, t_r) = scratch[9:]
    ep, tp, z, core, xn, yn, dg = places()
    n_z = n_ep // 2
    rows = o_ref.shape[0]
    cols = o_ref.shape[1]
    half = rows // 2
    other_core = z * 2 + 1 - core
    peers = (xn, yn, dg)
    greet(
        [(other_core, tp)]
        + [(((z + k) % n_z) * 2 + core, tp) for k in range(1, n_z)]
        + [(ep, t) for t in peers]
    )

    def send(src, dst, sem_s, sem_r, device):
        copy = pltpu.make_async_remote_copy(
            src_ref=src, dst_ref=dst, send_sem=sem_s, recv_sem=sem_r, device_id=device, device_id_type=MESH
        )
        copy.start()
        return copy

    order = list(range(2, n_z - 1)) + [1, n_z - 1, 0]
    c_copies, dx_copies, dy_copies, x_copies, y_copies, z_copies = {}, {}, {}, {}, {}, {}

    def down(k):
        pair = aligned((z + k) % n_z, 2 * rows)

        def tile(index, carry):
            part = aligned(index, cols)
            p[k, :, part] = jnp.dot(
                h_ref[pair, :], down_ref[:, part], preferred_element_type=jnp.float32
            ).astype(jnp.bfloat16)
            return carry

        lax.fori_loop(0, down_ref.shape[1] // cols, tile, 0)
        c_copies[k] = send(
            p.at[k, aligned(1 - core, rows), :], ca.at[k], c_s.at[k], c_r.at[k], (other_core, tp)
        )

    low, high = pl.ds(0, half), pl.ds(half, half)

    def first(k):
        c_copies[k].wait_recv()
        s[k] = (
            p[k, aligned(core, rows), :].astype(jnp.float32) + ca[k].astype(jnp.float32)
        ).astype(jnp.bfloat16)
        dx_copies[k] = send(
            s.at[k, low, aligned(dg, cols)], bx.at[k], dx_s.at[k], dx_r.at[k], (ep, xn)
        )
        dy_copies[k] = send(
            s.at[k, high, aligned(dg, cols)], by.at[k], dy_s.at[k], dy_r.at[k], (ep, yn)
        )

    def second(k):
        dx_copies[k].wait_recv()
        s[k, low, aligned(yn, cols)] = (
            s[k, low, aligned(yn, cols)].astype(jnp.float32) + bx[k].astype(jnp.float32)
        ).astype(jnp.bfloat16)
        y_copies[k] = send(
            s.at[k, :, aligned(yn, cols)], qy.at[k], y_s.at[k], y_r.at[k], (ep, yn)
        )
        dy_copies[k].wait_recv()
        s[k, high, aligned(xn, cols)] = (
            s[k, high, aligned(xn, cols)].astype(jnp.float32) + by[k].astype(jnp.float32)
        ).astype(jnp.bfloat16)
        x_copies[k] = send(
            s.at[k, :, aligned(xn, cols)], qx.at[k], x_s.at[k], x_r.at[k], (ep, xn)
        )

    def third(k):
        x_copies[k].wait_recv()
        y_copies[k].wait_recv()
        total = (
            s[k, :, aligned(tp, cols)].astype(jnp.float32)
            + qx[k].astype(jnp.float32)
            + qy[k].astype(jnp.float32)
        )
        if k == 0:
            o_ref[...] = total
        else:
            r[k] = total.astype(jnp.bfloat16)
            target = ((z + k) % n_z) * 2 + core
            z_copies[k] = send(r.at[k], bz.at[k], z_s.at[k], z_r.at[k], (target, tp))

    t_copies = []
    down(order[0])
    for index in range(n_z + 2):
        if index + 1 < n_z:
            down(order[index + 1])
        if index < n_z:
            first(order[index])
        if 1 <= index < n_z + 1:
            second(order[index - 1])
        if index == n_z:
            for number, t in enumerate(peers):
                pairs = (
                    (sh_ref, sh_all.at[:, aligned(tp, sh_ref.shape[1])]),
                    (po_ref, po_all.at[:, aligned(tp, po_ref.shape[1])]),
                    (sq_ref, sq_all.at[tp]),
                )
                for kind, (src, dst) in enumerate(pairs):
                    t_copies.append(
                        send(src, dst, t_s.at[number, kind], t_r.at[number, kind], (ep, t))
                    )
        if index >= 2:
            third(order[index - 2])
    sh_all[:, aligned(tp, sh_ref.shape[1])] = sh_ref[...]
    po_all[:, aligned(tp, po_ref.shape[1])] = po_ref[...]
    sq_all[tp] = sq_ref[...]
    for k in order[:-1]:
        z_copies[k].wait_recv()
        o_ref[...] += bz[k].astype(jnp.float32)
    for copy in t_copies:
        copy.wait()
    for group in (c_copies, dx_copies, dy_copies, x_copies, y_copies, z_copies):
        for copy in group.values():
            copy.wait_send()


def reduce_rows(hidden, down, shared_hidden, pooled, squares, n_ep, n_tp):
    n_z = n_ep // 2
    rows, width = hidden.shape[0] // n_ep, down.shape[1]
    cols = width // n_tp
    half = rows // 2
    bf16 = jnp.bfloat16
    vmem = pl.BlockSpec(memory_space=pltpu.VMEM)
    scratch = [
        pltpu.VMEM((n_z, 2 * rows, width), bf16),
        pltpu.VMEM((n_z, rows, width), bf16),
        pltpu.VMEM((n_z, rows, width), bf16),
        pltpu.VMEM((n_z, half, cols), bf16),
        pltpu.VMEM((n_z, half, cols), bf16),
        pltpu.VMEM((n_z, rows, cols), bf16),
        pltpu.VMEM((n_z, rows, cols), bf16),
        pltpu.VMEM((n_z, rows, cols), bf16),
        pltpu.VMEM((n_z, rows, cols), bf16),
    ]
    sems = [pltpu.SemaphoreType.DMA((n_z,))] * 12 + [pltpu.SemaphoreType.DMA((3, 3))] * 2
    return pl.pallas_call(
        lambda *refs: reduce_kernel(n_ep, *refs),
        out_shape=(
            jax.ShapeDtypeStruct((rows, cols), jnp.float32),
            jax.ShapeDtypeStruct((rows, n_tp * shared_hidden.shape[1]), bf16),
            jax.ShapeDtypeStruct((rows, n_tp * pooled.shape[1]), bf16),
            jax.ShapeDtypeStruct((n_tp,) + squares.shape, jnp.float32),
        ),
        in_specs=[vmem] * 5,
        out_specs=(vmem,) * 4,
        scratch_shapes=scratch + sems,
        compiler_params=pltpu.CompilerParams(
            collective_id=1, has_side_effects=True, vmem_limit_bytes=24 << 20
        ),
    )(hidden, down, shared_hidden, pooled, squares)


def dense_on_device(
    mix_input,
    expert_input,
    mix_gain,
    moe_gain,
    pool_in,
    pool_scale,
    pool_gain,
    pool_out,
    route,
    route_score,
    expert_gate,
    expert_up,
    expert_down,
    shared_gate,
    shared_up,
    shared_down,
):
    n_ep, n_tp = lax.axis_size("ep"), lax.axis_size("tp")
    me = lax.axis_index("ep")
    tok_rows = mix_input.shape[0]
    channels = pool_in.shape[1]
    pool_width = channels * n_tp
    f32 = jnp.float32

    moe_norm = row_norm(expert_input, moe_gain)
    weights = 2.5 * route_score / jnp.sum(route_score, axis=1, keepdims=True)
    experts = jnp.arange(n_ep, dtype=jnp.int32)
    dense = jnp.sum(
        jnp.where(route.T[None, :, :] == experts[:, None, None], weights.T[None, :, :], 0.0), axis=1
    )
    mix_norm = row_norm(mix_input, mix_gain)
    pool_input = jnp.dot(mix_norm, pool_in, preferred_element_type=f32).astype(jnp.bfloat16)
    before = shifted(pool_input[tok_rows - reach_rows :], "ep", 1)
    all_rows, all_weights, shared_hidden = gather_rows(
        moe_norm, dense, shared_gate, shared_up, n_ep
    )

    extended = jnp.concatenate([before, pool_input], axis=0).astype(f32)
    position = (me * tok_rows + jnp.arange(tok_rows, dtype=jnp.int32) + 1).astype(f32)
    channel_ids = lax.axis_index("tp") * channels + jnp.arange(channels, dtype=jnp.int32)
    group = channel_ids // (pool_width // 4)
    scaled = window_means(extended, position, group, tok_rows) * pool_scale
    squares = jnp.sum(scaled * scaled, axis=1)[None, :]
    pooled = (scaled * pool_gain).astype(jnp.bfloat16)
    factor = lax.dynamic_index_in_dim(all_weights, me, axis=1, keepdims=False).reshape(-1, 1)
    gate = jnp.dot(all_rows, expert_gate[0], preferred_element_type=f32)
    upper = jnp.dot(all_rows, expert_up[0], preferred_element_type=f32)
    hidden = (jax.nn.silu(gate) * upper * factor).astype(jnp.bfloat16)
    routed, shared_all, pooled_all, squares_all = reduce_rows(
        hidden, expert_down[0], shared_hidden, pooled, squares, n_ep, n_tp
    )
    mean = jnp.sum(squares_all, axis=0).reshape(-1, 1) / pool_width
    mix_out = (
        jnp.dot(pooled_all, pool_out, preferred_element_type=f32) * lax.rsqrt(mean + epsilon)
    ).astype(jnp.bfloat16)
    shared_part = jnp.dot(shared_all, shared_down, preferred_element_type=f32)
    return (mix_out, (routed + shared_part).astype(jnp.bfloat16))


def chosen(*arrays):
    route, expert_gate = arrays[8], arrays[10]
    experts = expert_gate.shape[0] * lax.axis_size("ep")
    capacity = 2 * route.shape[0] * route.shape[1] // experts
    square = lax.axis_size("tp") == 4 and lax.axis_size("ep") >= 6
    if capacity == route.shape[0] and expert_gate.shape[0] == 1 and square:
        return dense_on_device(*arrays)
    return on_device(*arrays)


def solution(mesh):
    return jax.shard_map(
        chosen,
        mesh=mesh,
        in_specs=(
            P("ep", None),
            P("ep", None),
            P(),
            P(),
            P(None, "tp"),
            P("tp"),
            P("tp"),
            P(None, "tp"),
            P("ep", None),
            P("ep", None),
            P("ep", None, "tp"),
            P("ep", None, "tp"),
            P("ep", "tp", None),
            P(None, "tp"),
            P(None, "tp"),
            P(None, "tp"),
        ),
        out_specs=(P("ep", "tp"), P("ep", "tp")),
        check_vma=False,
    )
```

```python
import jax
import jax.numpy as jnp
from jax import lax
from jax.experimental import pallas as pl
from jax.experimental.pallas import tpu as pltpu
from jax.sharding import PartitionSpec as P

epsilon = 1e-06
reach_rows = 15
window_widths = (2, 4, 8, 16)


def shifted(block, axis, distance):
    devices = range(lax.axis_size(axis))
    route = [(i - distance, i) for i in devices if i - distance in devices]
    return lax.ppermute(block, axis, route)


def row_norm(rows, gain):
    values = rows.astype(jnp.float32)
    scale = lax.rsqrt(jnp.mean(values * values, axis=-1, keepdims=True) + epsilon)
    return (values * scale * gain).astype(jnp.bfloat16)


def window_means(extended, position, group, n_rows):
    total = jnp.zeros((n_rows, extended.shape[1]), jnp.float32)
    result = jnp.zeros((n_rows, extended.shape[1]), jnp.float32)
    for lag in range(16):
        total = total + extended[reach_rows - lag : reach_rows - lag + n_rows]
        for index, width in enumerate(window_widths):
            if lag + 1 == width:
                count = jnp.minimum(position, float(width))[:, None]
                result = jnp.where(group[None, :] == index, total / count, result)
    return result - extended[reach_rows:]


def serve(sending, expert_gate, expert_up, expert_down):
    arrived = lax.all_to_all(sending, "ep", split_axis=0, concat_axis=0, tiled=True)
    gate = jnp.einsum("send,edf->senf", arrived, expert_gate, preferred_element_type=jnp.float32)
    upper = jnp.einsum("send,edf->senf", arrived, expert_up, preferred_element_type=jnp.float32)
    hidden = (jax.nn.silu(gate) * upper).astype(jnp.bfloat16)
    term = jnp.einsum("senf,efd->send", hidden, expert_down, preferred_element_type=jnp.float32)
    summed = lax.psum_scatter(term.astype(jnp.bfloat16), "tp", scatter_dimension=3, tiled=True)
    return lax.all_to_all(summed, "ep", split_axis=0, concat_axis=0, tiled=True)


def on_device(
    mix_input,
    expert_input,
    mix_gain,
    moe_gain,
    pool_in,
    pool_scale,
    pool_gain,
    pool_out,
    route,
    route_score,
    expert_gate,
    expert_up,
    expert_down,
    shared_gate,
    shared_up,
    shared_down,
):
    tok_rows = mix_input.shape[0]
    channels = pool_in.shape[1]
    pool_width = channels * lax.axis_size("tp")
    mix_norm = row_norm(mix_input, mix_gain)
    pool_input = jnp.dot(mix_norm, pool_in, preferred_element_type=jnp.float32).astype(jnp.bfloat16)
    before = shifted(pool_input[tok_rows - reach_rows :], "ep", 1)
    extended = jnp.concatenate([before, pool_input], axis=0).astype(jnp.float32)
    position = (lax.axis_index("ep") * tok_rows + jnp.arange(tok_rows, dtype=jnp.int32) + 1).astype(
        jnp.float32
    )
    channel_ids = lax.axis_index("tp") * channels + jnp.arange(channels, dtype=jnp.int32)
    group = channel_ids // (pool_width // 4)
    scaled = window_means(extended, position, group, tok_rows) * pool_scale
    squares = lax.psum(jnp.sum(scaled * scaled, axis=1), "tp")
    pooled_norm = (scaled * lax.rsqrt(squares / pool_width + epsilon)[:, None] * pool_gain).astype(
        jnp.bfloat16
    )
    moe_norm = row_norm(expert_input, moe_gain)
    shared_hidden = (
        jax.nn.silu(jnp.dot(moe_norm, shared_gate, preferred_element_type=jnp.float32))
        * jnp.dot(moe_norm, shared_up, preferred_element_type=jnp.float32)
    ).astype(jnp.bfloat16)
    pooled_all, shared_all = (
        lax.all_gather(pooled_norm, "tp", axis=1, tiled=True),
        lax.all_gather(shared_hidden, "tp", axis=1, tiled=True),
    )
    mix_out = jnp.dot(pooled_all, pool_out, preferred_element_type=jnp.float32).astype(jnp.bfloat16)
    shared_part = jnp.dot(shared_all, shared_down, preferred_element_type=jnp.float32)
    n_tok, top = route.shape
    local_experts = expert_gate.shape[0]
    experts = local_experts * lax.axis_size("ep")
    capacity = 2 * n_tok * top // experts
    flat_route = route.reshape(-1)
    table = (flat_route[:, None] == jnp.arange(experts, dtype=jnp.int32)[None, :]).astype(jnp.int32)
    ranks = jnp.sum((jnp.cumsum(table, axis=0) - table) * table, axis=1)
    slot = flat_route * capacity + ranks
    owner = (
        jnp.full((experts * capacity,), n_tok, jnp.int32)
        .at[slot]
        .set(jnp.arange(n_tok * top, dtype=jnp.int32) // top)
    )
    padded_rows = jnp.concatenate(
        [moe_norm, jnp.zeros((1, moe_norm.shape[1]), jnp.bfloat16)], axis=0
    )
    outgoing = padded_rows[owner].reshape(
        lax.axis_size("ep"), local_experts, capacity, moe_norm.shape[1]
    )
    middle = capacity // 2
    first = serve(outgoing[:, :, :middle], expert_gate, expert_up, expert_down)
    second = serve(outgoing[:, :, middle:], expert_gate, expert_up, expert_down)
    returned = jnp.concatenate([first, second], axis=2)
    back_rows = returned.reshape(experts * capacity, returned.shape[3])
    picked = back_rows[slot].reshape(n_tok, top, returned.shape[3]).astype(jnp.float32)
    weights = 2.5 * route_score / jnp.sum(route_score, axis=1, keepdims=True)
    routed = jnp.sum(picked * weights[:, :, None], axis=1)
    moe_out = (routed + shared_part).astype(jnp.bfloat16)
    return (mix_out, moe_out)


MESH = pl.DeviceIdType.MESH


def places():
    ep, tp = lax.axis_index("ep"), lax.axis_index("tp")
    z, core = ep // 2, ep % 2
    y, x = tp // 2, tp % 2
    return ep, tp, z, core, y * 2 + 1 - x, (1 - y) * 2 + x, (1 - y) * 2 + 1 - x


def greet(partners):
    barrier = pltpu.get_barrier_semaphore()
    for partner in partners:
        pl.semaphore_signal(barrier, inc=1, device_id=partner, device_id_type=MESH)
    pl.semaphore_wait(barrier, len(partners))


def aligned(start, size):
    return pl.ds(pl.multiple_of(start * size, size), size)


def gather_kernel(n_ep, m_ref, w_ref, sg_hbm, su_hbm, g_ref, wg_ref, sh_ref, *scratch):
    (w_s, w_r, z_s, z_r, x_s, x_r, y_s, y_r, dx_s, dx_r, dy_s, dy_r, c_s, c_r) = scratch[:14]
    sg_ref, su_ref, load = scratch[14:]
    loads = [
        pltpu.make_async_copy(sg_hbm, sg_ref, load.at[0]),
        pltpu.make_async_copy(su_hbm, su_ref, load.at[1]),
    ]
    for copy in loads:
        copy.start()
    ep, tp, z, core, xn, yn, _ = places()
    n_z = n_ep // 2
    rows = m_ref.shape[0]
    cols = m_ref.shape[1] // 4
    half = rows // 2
    greet([((ep + m) % n_ep, tp) for m in range(1, n_ep)] + [(ep, xn), (ep, yn)])

    def send(src, dst, s, r, device):
        copy = pltpu.make_async_remote_copy(
            src_ref=src, dst_ref=dst, send_sem=s, recv_sem=r, device_id=device, device_id_type=MESH
        )
        copy.start()
        return copy

    own_rows = aligned(ep, rows)
    other_core = z * 2 + 1 - core
    order = [k for k in (1, n_z - 1)] + list(range(2, n_z - 1))
    z_copies = {}
    for k in order:
        target = ((z + k) % n_z) * 2 + core
        z_copies[k] = send(
            m_ref.at[:, aligned(tp, cols)],
            g_ref.at[own_rows, aligned(tp, cols)],
            z_s.at[k],
            z_r.at[k],
            (target, tp),
        )
    c_copies = {0: send(m_ref, g_ref.at[own_rows, :], c_s.at[0], c_r.at[0], (other_core, tp))}
    w_copies = [
        send(w_ref, wg_ref.at[ep], w_s.at[m], w_r.at[m], ((ep + m) % n_ep, tp))
        for m in range(1, n_ep)
    ]
    g_ref[own_rows, :] = m_ref[...]
    wg_ref[ep] = w_ref[...]
    tile = sg_ref.shape[1] // 2

    def shared_tile(index, carry):
        part = aligned(index, tile)
        gate = jnp.dot(m_ref[...], sg_ref[:, part], preferred_element_type=jnp.float32)
        upper = jnp.dot(m_ref[...], su_ref[:, part], preferred_element_type=jnp.float32)
        sh_ref[:, part] = (gate / (1.0 + jnp.exp(-gate)) * upper).astype(jnp.bfloat16)
        return carry

    for copy in loads:
        copy.wait()
    lax.fori_loop(0, 2, shared_tile, 0)
    x_copies, y_copies, dx_copies, dy_copies = {}, {}, {}, {}

    def block(k):
        return ((z + n_z - k) % n_z) * 2 + core

    def piece(k, quarter):
        return g_ref.at[aligned(block(k), rows), aligned(quarter, cols)]

    def half_piece(k, part, quarter):
        start = pl.multiple_of(block(k) * rows + part * half, half)
        return g_ref.at[pl.ds(start, half), aligned(quarter, cols)]

    def across(k):
        z_copies[k].wait_recv()
        x_copies[k] = send(piece(k, tp), piece(k, tp), x_s.at[k], x_r.at[k], (ep, xn))
        y_copies[k] = send(piece(k, tp), piece(k, tp), y_s.at[k], y_r.at[k], (ep, yn))

    def corner(k):
        x_copies[k].wait_recv()
        dx_copies[k] = send(
            half_piece(k, 0, xn), half_piece(k, 0, xn), dx_s.at[k], dx_r.at[k], (ep, yn)
        )
        y_copies[k].wait_recv()
        dy_copies[k] = send(
            half_piece(k, 1, yn), half_piece(k, 1, yn), dy_s.at[k], dy_r.at[k], (ep, xn)
        )

    def over(k):
        dx_copies[k].wait_recv()
        dy_copies[k].wait_recv()
        whole = g_ref.at[aligned(block(k), rows), :]
        c_copies[k] = send(whole, whole, c_s.at[k], c_r.at[k], (other_core, tp))

    for index in range(len(order) + 2):
        if index < len(order):
            across(order[index])
        if 1 <= index < len(order) + 1:
            corner(order[index - 1])
        if index >= 2:
            over(order[index - 2])
    for k in [0] + order:
        c_copies[k].wait_recv()
    for copy in w_copies:
        copy.wait()
    for group in (z_copies, x_copies, y_copies, dx_copies, dy_copies, c_copies):
        for copy in group.values():
            copy.wait_send()


def gather_rows(moe_norm, dense, shared_gate, shared_up, n_ep):
    n_z = n_ep // 2
    sems = [pltpu.SemaphoreType.DMA((n_ep,))] * 2 + [pltpu.SemaphoreType.DMA((n_z,))] * 12
    sems = sems + [
        pltpu.VMEM(shared_gate.shape, jnp.bfloat16),
        pltpu.VMEM(shared_up.shape, jnp.bfloat16),
        pltpu.SemaphoreType.DMA((2,)),
    ]
    vmem = pl.BlockSpec(memory_space=pltpu.VMEM)
    return pl.pallas_call(
        lambda *refs: gather_kernel(n_ep, *refs),
        out_shape=(
            jax.ShapeDtypeStruct((n_ep * moe_norm.shape[0], moe_norm.shape[1]), jnp.bfloat16),
            jax.ShapeDtypeStruct((n_ep,) + dense.shape, jnp.float32),
            jax.ShapeDtypeStruct((moe_norm.shape[0], shared_gate.shape[1]), jnp.bfloat16),
        ),
        in_specs=[vmem] * 2 + [pl.BlockSpec(memory_space=pltpu.HBM)] * 2,
        out_specs=(vmem,) * 3,
        scratch_shapes=sems,
        compiler_params=pltpu.CompilerParams(collective_id=0, has_side_effects=True, vmem_limit_bytes=20 << 20),
    )(moe_norm, dense, shared_gate, shared_up)


def reduce_kernel(n_ep, h_ref, down_ref, sh_ref, po_ref, sq_ref, o_ref, sh_all, po_all, sq_all, *scratch):
    (p, ca, s, bx, by, qx, qy, r, bz) = scratch[:9]
    (c_s, c_r, dx_s, dx_r, dy_s, dy_r, x_s, x_r, y_s, y_r, z_s, z_r, t_s, t_r) = scratch[9:]
    ep, tp, z, core, xn, yn, dg = places()
    n_z = n_ep // 2
    rows = o_ref.shape[0]
    cols = o_ref.shape[1]
    half = rows // 2
    other_core = z * 2 + 1 - core
    peers = (xn, yn, dg)
    greet(
        [(other_core, tp)]
        + [(((z + k) % n_z) * 2 + core, tp) for k in range(1, n_z)]
        + [(ep, t) for t in peers]
    )

    def send(src, dst, sem_s, sem_r, device):
        copy = pltpu.make_async_remote_copy(
            src_ref=src, dst_ref=dst, send_sem=sem_s, recv_sem=sem_r, device_id=device, device_id_type=MESH
        )
        copy.start()
        return copy

    order = list(range(2, n_z - 1)) + [1, n_z - 1, 0]
    c_copies, dx_copies, dy_copies, x_copies, y_copies, z_copies = {}, {}, {}, {}, {}, {}

    def down(k):
        pair = aligned((z + k) % n_z, 2 * rows)

        def tile(index, carry):
            part = aligned(index, cols)
            p[k, :, part] = jnp.dot(
                h_ref[pair, :], down_ref[:, part], preferred_element_type=jnp.float32
            ).astype(jnp.bfloat16)
            return carry

        lax.fori_loop(0, down_ref.shape[1] // cols, tile, 0)
        c_copies[k] = send(
            p.at[k, aligned(1 - core, rows), :], ca.at[k], c_s.at[k], c_r.at[k], (other_core, tp)
        )

    low, high = pl.ds(0, half), pl.ds(half, half)

    def first(k):
        c_copies[k].wait_recv()
        s[k] = (
            p[k, aligned(core, rows), :].astype(jnp.float32) + ca[k].astype(jnp.float32)
        ).astype(jnp.bfloat16)
        dx_copies[k] = send(
            s.at[k, low, aligned(dg, cols)], bx.at[k], dx_s.at[k], dx_r.at[k], (ep, xn)
        )
        dy_copies[k] = send(
            s.at[k, high, aligned(dg, cols)], by.at[k], dy_s.at[k], dy_r.at[k], (ep, yn)
        )

    def second(k):
        dx_copies[k].wait_recv()
        s[k, low, aligned(yn, cols)] = (
            s[k, low, aligned(yn, cols)].astype(jnp.float32) + bx[k].astype(jnp.float32)
        ).astype(jnp.bfloat16)
        y_copies[k] = send(
            s.at[k, :, aligned(yn, cols)], qy.at[k], y_s.at[k], y_r.at[k], (ep, yn)
        )
        dy_copies[k].wait_recv()
        s[k, high, aligned(xn, cols)] = (
            s[k, high, aligned(xn, cols)].astype(jnp.float32) + by[k].astype(jnp.float32)
        ).astype(jnp.bfloat16)
        x_copies[k] = send(
            s.at[k, :, aligned(xn, cols)], qx.at[k], x_s.at[k], x_r.at[k], (ep, xn)
        )

    def third(k):
        x_copies[k].wait_recv()
        y_copies[k].wait_recv()
        total = (
            s[k, :, aligned(tp, cols)].astype(jnp.float32)
            + qx[k].astype(jnp.float32)
            + qy[k].astype(jnp.float32)
        )
        if k == 0:
            o_ref[...] = total
        else:
            r[k] = total.astype(jnp.bfloat16)
            target = ((z + k) % n_z) * 2 + core
            z_copies[k] = send(r.at[k], bz.at[k], z_s.at[k], z_r.at[k], (target, tp))

    t_copies = []
    down(order[0])
    for index in range(n_z + 2):
        if index + 1 < n_z:
            down(order[index + 1])
        if index < n_z:
            first(order[index])
        if 1 <= index < n_z + 1:
            second(order[index - 1])
        if index == n_z:
            for number, t in enumerate(peers):
                pairs = (
                    (sh_ref, sh_all.at[:, aligned(tp, sh_ref.shape[1])]),
                    (po_ref, po_all.at[:, aligned(tp, po_ref.shape[1])]),
                    (sq_ref, sq_all.at[tp]),
                )
                for kind, (src, dst) in enumerate(pairs):
                    t_copies.append(
                        send(src, dst, t_s.at[number, kind], t_r.at[number, kind], (ep, t))
                    )
        if index >= 2:
            third(order[index - 2])
    sh_all[:, aligned(tp, sh_ref.shape[1])] = sh_ref[...]
    po_all[:, aligned(tp, po_ref.shape[1])] = po_ref[...]
    sq_all[tp] = sq_ref[...]
    for k in order[:-1]:
        z_copies[k].wait_recv()
        o_ref[...] += bz[k].astype(jnp.float32)
    for copy in t_copies:
        copy.wait()
    for group in (c_copies, dx_copies, dy_copies, x_copies, y_copies, z_copies):
        for copy in group.values():
            copy.wait_send()


def reduce_rows(hidden, down, shared_hidden, pooled, squares, n_ep, n_tp):
    n_z = n_ep // 2
    rows, width = hidden.shape[0] // n_ep, down.shape[1]
    cols = width // n_tp
    half = rows // 2
    bf16 = jnp.bfloat16
    vmem = pl.BlockSpec(memory_space=pltpu.VMEM)
    scratch = [
        pltpu.VMEM((n_z, 2 * rows, width), bf16),
        pltpu.VMEM((n_z, rows, width), bf16),
        pltpu.VMEM((n_z, rows, width), bf16),
        pltpu.VMEM((n_z, half, cols), bf16),
        pltpu.VMEM((n_z, half, cols), bf16),
        pltpu.VMEM((n_z, rows, cols), bf16),
        pltpu.VMEM((n_z, rows, cols), bf16),
        pltpu.VMEM((n_z, rows, cols), bf16),
        pltpu.VMEM((n_z, rows, cols), bf16),
    ]
    sems = [pltpu.SemaphoreType.DMA((n_z,))] * 12 + [pltpu.SemaphoreType.DMA((3, 3))] * 2
    return pl.pallas_call(
        lambda *refs: reduce_kernel(n_ep, *refs),
        out_shape=(
            jax.ShapeDtypeStruct((rows, cols), jnp.float32),
            jax.ShapeDtypeStruct((rows, n_tp * shared_hidden.shape[1]), bf16),
            jax.ShapeDtypeStruct((rows, n_tp * pooled.shape[1]), bf16),
            jax.ShapeDtypeStruct((n_tp,) + squares.shape, jnp.float32),
        ),
        in_specs=[vmem] * 5,
        out_specs=(vmem,) * 4,
        scratch_shapes=scratch + sems,
        compiler_params=pltpu.CompilerParams(
            collective_id=1, has_side_effects=True, vmem_limit_bytes=24 << 20
        ),
    )(hidden, down, shared_hidden, pooled, squares)


def dense_on_device(
    mix_input,
    expert_input,
    mix_gain,
    moe_gain,
    pool_in,
    pool_scale,
    pool_gain,
    pool_out,
    route,
    route_score,
    expert_gate,
    expert_up,
    expert_down,
    shared_gate,
    shared_up,
    shared_down,
):
    n_ep, n_tp = lax.axis_size("ep"), lax.axis_size("tp")
    me = lax.axis_index("ep")
    tok_rows = mix_input.shape[0]
    channels = pool_in.shape[1]
    pool_width = channels * n_tp
    f32 = jnp.float32

    moe_norm = row_norm(expert_input, moe_gain)
    weights = 2.5 * route_score / jnp.sum(route_score, axis=1, keepdims=True)
    experts = jnp.arange(n_ep, dtype=jnp.int32)
    dense = jnp.sum(
        jnp.where(route.T[None, :, :] == experts[:, None, None], weights.T[None, :, :], 0.0), axis=1
    )
    mix_norm = row_norm(mix_input, mix_gain)
    pool_input = jnp.dot(mix_norm, pool_in, preferred_element_type=f32).astype(jnp.bfloat16)
    before = shifted(pool_input[tok_rows - reach_rows :], "ep", 1)
    all_rows, all_weights, shared_hidden = gather_rows(
        moe_norm, dense, shared_gate, shared_up, n_ep
    )

    extended = jnp.concatenate([before, pool_input], axis=0).astype(f32)
    position = (me * tok_rows + jnp.arange(tok_rows, dtype=jnp.int32) + 1).astype(f32)
    channel_ids = lax.axis_index("tp") * channels + jnp.arange(channels, dtype=jnp.int32)
    group = channel_ids // (pool_width // 4)
    scaled = window_means(extended, position, group, tok_rows) * pool_scale
    squares = jnp.sum(scaled * scaled, axis=1)[None, :]
    pooled = (scaled * pool_gain).astype(jnp.bfloat16)
    factor = lax.dynamic_index_in_dim(all_weights, me, axis=1, keepdims=False).reshape(-1, 1)
    gate = jnp.dot(all_rows, expert_gate[0], preferred_element_type=f32)
    upper = jnp.dot(all_rows, expert_up[0], preferred_element_type=f32)
    hidden = (jax.nn.silu(gate) * upper * factor).astype(jnp.bfloat16)
    routed, shared_all, pooled_all, squares_all = reduce_rows(
        hidden, expert_down[0], shared_hidden, pooled, squares, n_ep, n_tp
    )
    mean = jnp.sum(squares_all, axis=0).reshape(-1, 1) / pool_width
    mix_out = (
        jnp.dot(pooled_all, pool_out, preferred_element_type=f32) * lax.rsqrt(mean + epsilon)
    ).astype(jnp.bfloat16)
    shared_part = jnp.dot(shared_all, shared_down, preferred_element_type=f32)
    return (mix_out, (routed + shared_part).astype(jnp.bfloat16))


def chosen(*arrays):
    route, expert_gate = arrays[8], arrays[10]
    experts = expert_gate.shape[0] * lax.axis_size("ep")
    capacity = 2 * route.shape[0] * route.shape[1] // experts
    square = lax.axis_size("tp") == 4 and lax.axis_size("ep") >= 6
    if capacity == route.shape[0] and expert_gate.shape[0] == 1 and square:
        return dense_on_device(*arrays)
    return on_device(*arrays)


def solution(mesh):
    return jax.shard_map(
        chosen,
        mesh=mesh,
        in_specs=(
            P("ep", None),
            P("ep", None),
            P(),
            P(),
            P(None, "tp"),
            P("tp"),
            P("tp"),
            P(None, "tp"),
            P("ep", None),
            P("ep", None),
            P("ep", None, "tp"),
            P("ep", None, "tp"),
            P("ep", "tp", None),
            P(None, "tp"),
            P(None, "tp"),
            P(None, "tp"),
        ),
        out_specs=(P("ep", "tp"), P("ep", "tp")),
        check_vma=False,
    )
```
